512 devices in a mesh: sp: 64 (over z, y), tp: 8 (over x, core).
Axes of the slice: x: 4, y: 4, z: 16, core: 2. Of those that a mesh axis runs over, the one named last changes fastest.
Arguments:
- tokens: bfloat16 [16384, 2048], P('sp'), may hold values from -6 to 6
- ln_gain: float32 [2048], replicated, may hold values from 0.1 to 1.9
- w_query_attn: bfloat16 [2048, 1024], P('sp', 'tp'), may hold values from -0.125 to 0.125
- w_key_attn: bfloat16 [2048, 1024], P('sp', 'tp'), may hold values from -0.125 to 0.125
- w_value_attn: bfloat16 [2048, 1024], P('sp', 'tp'), may hold values from -0.125 to 0.125
- w_query_delta: bfloat16 [2048, 1024], P('sp', 'tp'), may hold values from -0.125 to 0.125
- w_key_delta: bfloat16 [2048, 1024], P('sp', 'tp'), may hold values from -0.125 to 0.125
- w_value_delta: bfloat16 [2048, 1024], P('sp', 'tp'), may hold values from -0.125 to 0.125
- w_beta: bfloat16 [2048, 8], replicated, may hold values from -0.125 to 0.125
- w_decay: bfloat16 [2048, 8], replicated, may hold values from -0.125 to 0.125
- attn_bias: float32 [16], replicated, may hold values from -13 to 1
- decay_log: float32 [8], replicated, may hold values from -15 to -2
- beta_bias: float32 [8], replicated, may hold values from -7 to 1
- log_decay_extra: float32 [16384, 8], P('sp', 'tp'), may hold values from -0.7 to 0, as said below
- attn_gain: float32 [64], replicated, may hold values from 0.1 to 1.9
- delta_gain: float32 [128], replicated, may hold values from 0.1 to 1.9
- w_out_attn: bfloat16 [1024, 2048], P('tp', 'sp'), may hold values from -0.125 to 0.125
- w_out_delta: bfloat16 [1024, 2048], P('tp', 'sp'), may hold values from -0.125 to 0.125
Outputs:
- mixed_out: bfloat16 [16384, 2048], P(('sp', 'tp'))
The draws below stay inside these ranges and needn't reach their ends.
Inputs may be any that keep to these rules, and one draw needn't show every extreme that they name: `log_decay_extra`: never positive.
All inputs are finite; a program needn't handle non-finite values.
Results may differ from the reference program's by a relative error of at most 0.015.
Values may be sent and summed in bfloat16 or wider, within the bound.
A program may use at most 128 MiB of HBM per device.

```python
import math
import jax
import jax.numpy as jnp
from jax import lax

D = 2048
SB_HEADS = 16
SB_DIM = 64
GDN_HEADS = 8
GDN_DIM = 128
DBLOCK = 64
TOK_DEV = 256
SEQ = 16384
N_SP = 64
N_TP = 8


def draw_attn_bias(key, part):
    perm_key, level_key = jax.random.split(jax.random.fold_in(key, 11))
    ranks = jax.random.permutation(perm_key, SB_HEADS)
    slower = ranks < SB_HEADS // 2
    levels = jax.random.uniform(level_key, (SB_HEADS,), jnp.float32)
    far_reach = -jnp.log(jnp.float32(SEQ)) - 1.5 + 1.5 * levels
    near_reach = -jnp.log(jnp.float32(40.0)) - 1.0 + 2.0 * levels
    return jnp.where(slower, far_reach, near_reach).astype(jnp.float32)


def delta_heads(key):
    perm_key, first_key, second_key = jax.random.split(jax.random.fold_in(key, 23), 3)
    ranks = jax.random.permutation(perm_key, GDN_HEADS)
    slower = ranks < GDN_HEADS // 2
    first_level = jax.random.uniform(first_key, (GDN_HEADS,), jnp.float32)
    second_level = jax.random.uniform(second_key, (GDN_HEADS,), jnp.float32)
    return (slower, first_level, second_level)


def draw_decay_log(key, part):
    slower, first_level, second_level = delta_heads(key)
    slow_rate = jnp.log(0.05 + 0.15 * first_level) - jnp.log(jnp.float32(SEQ))
    fast_rate = jnp.log(0.03 + 0.07 * first_level)
    return jnp.where(slower, slow_rate, fast_rate).astype(jnp.float32)


def draw_beta_bias(key, part):
    slower, first_level, second_level = delta_heads(key)
    return jnp.where(slower, -7.0 + second_level, -1.0 + 2.0 * second_level).astype(jnp.float32)


def draw_log_decay_extra(key, part):
    rate_key, location_key, drop_key = jax.random.split(jax.random.fold_in(key, 37), 3)
    rates = jnp.exp(jax.random.uniform(rate_key, (N_SP, GDN_HEADS), jnp.float32, jnp.log(0.4), jnp.log(1.2))) / SEQ
    base = -jnp.repeat(rates, TOK_DEV, axis=0)
    quarter = SEQ // 4
    spots = jax.random.randint(location_key, (4, GDN_HEADS), 0, quarter)
    spots = spots + (jnp.arange(4, dtype=jnp.int32) * quarter)[:, None]
    drops = jnp.log(jax.random.uniform(drop_key, (4, GDN_HEADS), jnp.float32, 0.5, 0.6))
    positions = jnp.arange(SEQ, dtype=jnp.int32)[:, None]
    result = base
    for which in range(4):
        result = result + jnp.where(positions == spots[which][None, :], drops[which][None, :], 0.0)
    return jnp.maximum(result, -0.7).astype(jnp.float32)


def shard_levels(stream_key, shape, pieces, smallest, largest):
    def one(position, blocks):
        draws = jax.random.uniform(jax.random.fold_in(jax.random.fold_in(stream_key, 6), position), (blocks,), jnp.float32, smallest / len(pieces), largest / len(pieces))
        return jnp.repeat(jnp.exp(draws), shape[position] // blocks).reshape((-1,) + (1,) * (len(shape) - position - 1))

    loudness = one(*pieces[0])
    for cut in pieces[1:]:
        loudness = loudness * one(*cut)
    return loudness


def centred(own_key, dims, scale, most, pieces=(), held_as=jnp.bfloat16):
    factor_of = shard_levels(own_key, dims, pieces, -0.22, 0.18) if pieces else 1.0
    drawn = jax.random.normal(own_key, dims, jnp.float32) * scale * factor_of
    return jnp.minimum(jnp.maximum(drawn, -most), most).astype(held_as)


def setup_inputs(seed: int = 0) -> dict:
    key_list = jax.random.split(jax.random.key(seed), 19)
    tokens = centred(key_list[0], (SEQ, D), 1.0, 6.0, ((0, 64),))
    ln_gain = jnp.clip(1.0 + 0.18 * jax.random.normal(key_list[1], (D,), jnp.float32), 0.1, 1.9)
    w_query_attn = centred(key_list[2], (D, SB_HEADS * SB_DIM), D ** -0.5, 0.125, ((0, 64), (1, 8)))
    w_key_attn = centred(key_list[3], (D, SB_HEADS * SB_DIM), D ** -0.5, 0.125, ((0, 64), (1, 8)))
    w_value_attn = centred(key_list[4], (D, SB_HEADS * SB_DIM), D ** -0.5, 0.125, ((0, 64), (1, 8)))
    w_query_delta = centred(key_list[5], (D, GDN_HEADS * GDN_DIM), D ** -0.5, 0.125, ((0, 64), (1, 8)))
    w_key_delta = centred(key_list[6], (D, GDN_HEADS * GDN_DIM), D ** -0.5, 0.125, ((0, 64), (1, 8)))
    w_value_delta = centred(key_list[7], (D, GDN_HEADS * GDN_DIM), D ** -0.5, 0.125, ((0, 64), (1, 8)))
    w_beta = centred(key_list[8], (D, GDN_HEADS), D ** -0.5, 0.125)
    w_decay = centred(key_list[9], (D, GDN_HEADS), D ** -0.5, 0.125)
    attn_bias = draw_attn_bias(jax.random.fold_in(key_list[18], 71), 0)
    decay_log = draw_decay_log(jax.random.fold_in(key_list[18], 71), 0)
    beta_bias = draw_beta_bias(jax.random.fold_in(key_list[18], 71), 0)
    log_decay_extra = draw_log_decay_extra(jax.random.fold_in(key_list[18], 71), 0)
    attn_gain = jnp.clip(1.0 + 0.18 * jax.random.normal(key_list[14], (SB_DIM,), jnp.float32), 0.1, 1.9)
    delta_gain = jnp.clip(1.0 + 0.18 * jax.random.normal(key_list[15], (GDN_DIM,), jnp.float32), 0.1, 1.9)
    w_out_attn = centred(key_list[16], (SB_HEADS * SB_DIM, D), (SB_HEADS * SB_DIM + GDN_HEADS * GDN_DIM) ** -0.5, 0.125, ((0, 8), (1, 64)))
    w_out_delta = centred(key_list[17], (GDN_HEADS * GDN_DIM, D), (SB_HEADS * SB_DIM + GDN_HEADS * GDN_DIM) ** -0.5, 0.125, ((0, 8), (1, 64)))
    return {"tokens": tokens, "ln_gain": ln_gain, "w_query_attn": w_query_attn, "w_key_attn": w_key_attn, "w_value_attn": w_value_attn, "w_query_delta": w_query_delta, "w_key_delta": w_key_delta, "w_value_delta": w_value_delta, "w_beta": w_beta, "w_decay": w_decay, "attn_bias": attn_bias, "decay_log": decay_log, "beta_bias": beta_bias, "log_decay_extra": log_decay_extra, "attn_gain": attn_gain, "delta_gain": delta_gain, "w_out_attn": w_out_attn, "w_out_delta": w_out_delta}


precise = lax.Precision.HIGHEST

def layer_normed(tok_rows, ln_gain):
    values = tok_rows.astype(jnp.float32)
    center = lax.optimization_barrier(jnp.mean(values, axis=-1, keepdims=True))
    spread = lax.optimization_barrier(jnp.mean(jnp.square(values - center), axis=-1, keepdims=True))
    return ((values - center) * lax.rsqrt(spread + 1e-05) * ln_gain).astype(jnp.bfloat16)

def rms_scaled(values, gain):
    return values * lax.rsqrt(lax.optimization_barrier(jnp.mean(jnp.square(values), axis=-1, keepdims=True)) + 1e-06) * gain

def unit_rows(values):
    return values * lax.rsqrt(lax.optimization_barrier(jnp.sum(jnp.square(values), axis=-1, keepdims=True)) + 1e-06)

def stick_block(carry, queries, query_pos, head_bias, key_block, value_block, key_first):
    outputs, log_kept = carry
    key_count = key_block.shape[0]
    heads = queries.shape[1]
    head_width = queries.shape[2]
    scores = jnp.einsum('rhd,khd->hrk', queries.astype(jnp.float32), key_block.reshape(key_count, heads, head_width).astype(jnp.float32))
    scores = scores * head_width ** (-0.5) + head_bias[:, None, None]
    key_pos = key_first + jnp.arange(key_count, dtype=jnp.int32)
    visible = (key_pos[None, :] < query_pos[:, None]) & (key_pos[None, :] >= 0)
    lost = jnp.where(visible[None], -jax.nn.softplus(scores), 0.0)
    between = lax.cumsum(lost, axis=2, reverse=True) - lost + log_kept[:, :, None]
    weights = jnp.where(visible[None], jnp.exp(jax.nn.log_sigmoid(scores) + between), 0.0)
    rounded = lax.optimization_barrier(weights.astype(jnp.bfloat16)).astype(jnp.float32)
    outputs = outputs + jnp.einsum('hrk,khd->hrd', rounded, value_block.reshape(key_count, heads, head_width).astype(jnp.float32))
    return (outputs, log_kept + lax.optimization_barrier(jnp.sum(lost, axis=2)))

def stick_attention(queries, keys, values, head_bias):
    grand_sum = queries.shape[0]
    heads = queries.shape[1]
    head_width = queries.shape[2]
    block = math.gcd(1024, grand_sum)
    blocks = grand_sum // block

    def query_block(index):
        first_pos = (index * block).astype(jnp.int32)
        block_queries = lax.dynamic_slice_in_dim(queries, first_pos, block, 0)
        query_pos = first_pos + jnp.arange(block, dtype=jnp.int32)

        def one_turn(step_index, carry):
            key_first = ((index - step_index) * block).astype(jnp.int32)
            key_block = lax.dynamic_slice_in_dim(keys, key_first, block, 0)
            value_block = lax.dynamic_slice_in_dim(values, key_first, block, 0)
            return stick_block(carry, block_queries, query_pos, head_bias, key_block, value_block, key_first)
        initial_carry = (jnp.zeros((heads, block, head_width), jnp.float32), jnp.zeros((heads, block), jnp.float32))
        outputs, _ = lax.fori_loop(0, index + 1, one_turn, initial_carry)
        return outputs
    results = lax.map(query_block, jnp.arange(blocks, dtype=jnp.int32))
    return jnp.moveaxis(results, 0, 1).reshape(heads, grand_sum, head_width)

def delta_parts(queries, keys, values, beta, decay):
    width = queries.shape[-2]
    key_width = queries.shape[-1]
    decay_sum = jnp.cumsum(decay, axis=-1)
    lower = jnp.tril(jnp.ones((width, width), dtype=bool))
    strict = jnp.tril(jnp.ones((width, width), dtype=bool), -1)
    differ = decay_sum[..., :, None] - decay_sum[..., None, :]
    decay_mask = jnp.where(lower, jnp.exp(jnp.where(lower, differ, 0.0)), 0.0)
    keys_beta = keys * beta[..., None]
    values_beta = values * beta[..., None]
    strict_mat = jnp.where(strict, jnp.einsum('...id,...jd->...ij', keys_beta, keys, precision=precise) * decay_mask, 0.0)
    right_side = jnp.concatenate([keys_beta * jnp.exp(decay_sum)[..., None], values_beta], axis=-1)
    solved = jax.scipy.linalg.solve_triangular(jnp.eye(width, dtype=jnp.float32) + strict_mat, right_side, lower=True)
    solve_keys = solved[..., :key_width]
    solve_values = solved[..., key_width:]
    query_key = jnp.einsum('...id,...jd->...ij', queries, keys, precision=precise) * decay_mask
    query_decayed = queries * jnp.exp(decay_sum)[..., None]
    keys_to_end = keys * jnp.exp(decay_sum[..., -1:] - decay_sum)[..., None]
    block_decay = jnp.exp(decay_sum[..., -1])
    return (solve_keys, solve_values, query_decayed, query_key, keys_to_end, block_decay)

def delta_update(state, block_parts):
    solve_keys, solve_values, query_decayed, query_key, keys_to_end, block_decay = block_parts
    fresh = solve_values - jnp.einsum('hcd,hde->hce', solve_keys, state, precision=precise)
    outputs = jnp.einsum('hcd,hde->hce', query_decayed, state, precision=precise)
    outputs = outputs + jnp.einsum('hij,hje->hie', query_key, fresh, precision=precise)
    state = state * block_decay[:, None, None] + jnp.einsum('hcd,hce->hde', keys_to_end, fresh, precision=precise)
    return (state, outputs)

def delta_attention(queries, keys, values, beta, decay):
    length = queries.shape[0]
    heads = queries.shape[1]
    blocks = length // DBLOCK

    def to_blocks(array):
        return jnp.moveaxis(array.reshape((blocks, DBLOCK) + array.shape[1:]), 2, 0)
    parts = delta_parts(to_blocks(queries), to_blocks(keys), to_blocks(values), to_blocks(beta), to_blocks(decay))
    sequence = tuple((jnp.moveaxis(piece_part, 1, 0) for piece_part in parts))
    start_state = jnp.zeros((heads, queries.shape[2], values.shape[2]), jnp.float32)
    _, outputs = lax.scan(delta_update, start_state, sequence)
    return jnp.moveaxis(outputs, 0, 1).reshape(heads, length, values.shape[2])

def reference(tokens, ln_gain, w_query_attn, w_key_attn, w_value_attn, w_query_delta, w_key_delta, w_value_delta, w_beta, w_decay, attn_bias, decay_log, beta_bias, log_decay_extra, attn_gain, delta_gain, w_out_attn, w_out_delta):
    normed = layer_normed(tokens, ln_gain)
    length = tokens.shape[0]

    def project(weight):
        return jnp.dot(normed.astype(jnp.float32), weight.astype(jnp.float32), preferred_element_type=jnp.float32).astype(jnp.bfloat16)
    attn_query = project(w_query_attn).reshape(length, SB_HEADS, SB_DIM)
    attn_key = project(w_key_attn)
    attn_value = project(w_value_attn)
    delta_query = project(w_query_delta)
    delta_key = project(w_key_delta)
    delta_value = project(w_value_delta)
    beta_pre = project(w_beta)
    decay_pre = project(w_decay)
    attn_raw = stick_attention(attn_query, attn_key, attn_value, attn_bias)
    attn_mixed = rms_scaled(attn_raw, attn_gain).astype(jnp.bfloat16)
    queries = unit_rows(jax.nn.silu(delta_query.astype(jnp.float32)).reshape(length, GDN_HEADS, GDN_DIM)) * GDN_DIM ** (-0.5)
    keys = unit_rows(jax.nn.silu(delta_key.astype(jnp.float32)).reshape(length, GDN_HEADS, GDN_DIM))
    values = jax.nn.silu(delta_value.astype(jnp.float32)).reshape(length, GDN_HEADS, GDN_DIM)
    beta = jax.nn.sigmoid(beta_pre.astype(jnp.float32) + beta_bias)
    decay = -jnp.exp(decay_log) * jax.nn.softplus(decay_pre.astype(jnp.float32)) + log_decay_extra
    delta_raw = delta_attention(queries, keys, values, beta, decay)
    delta_mixed = rms_scaled(delta_raw, delta_gain).astype(jnp.bfloat16)
    attn_group = SB_HEADS // N_TP
    delta_group = GDN_HEADS // N_TP
    summed = jnp.zeros((length, w_out_attn.shape[1]), jnp.float32)
    for group in range(N_TP):
        attn_cols = jnp.transpose(attn_mixed[group * attn_group:(group + 1) * attn_group], (1, 0, 2)).reshape(length, attn_group * SB_DIM)
        delta_cols = jnp.transpose(delta_mixed[group * delta_group:(group + 1) * delta_group], (1, 0, 2)).reshape(length, delta_group * GDN_DIM)
        partial_sum = jnp.dot(attn_cols.astype(jnp.float32), w_out_attn[group * attn_group * SB_DIM:(group + 1) * attn_group * SB_DIM].astype(jnp.float32), preferred_element_type=jnp.float32)
        partial_sum = partial_sum + jnp.dot(delta_cols.astype(jnp.float32), w_out_delta[group * delta_group * GDN_DIM:(group + 1) * delta_group * GDN_DIM].astype(jnp.float32), preferred_element_type=jnp.float32)
        summed = summed + lax.optimization_barrier(partial_sum.astype(jnp.bfloat16)).astype(jnp.float32)
    return summed.astype(jnp.bfloat16)
```

```python
import functools

import jax
import jax.numpy as jnp
from jax import lax
from jax.experimental import pallas as pl
from jax.experimental.pallas import tpu as pltpu
from jax.sharding import Mesh
from jax.sharding import PartitionSpec as P

MESH = pl.DeviceIdType.MESH
VMEM = pltpu.VMEM
SP = ("z", "y")
LOG2E = 1.4426950408889634
ROWS = 256
F32 = jnp.float32
BF16 = jnp.bfloat16
HIGH = lax.Precision.HIGHEST


def dot(a, b, dims=((1,), (0,)), precision=None):
    return lax.dot_general(
        a, b, (dims, ((), ())), precision=precision, preferred_element_type=F32
    )


def exact(a, b, dims=((1,), (0,))):
    return dot(a, b, dims, HIGH)


def vmem_call(body, outs, scratch=(), smem=0, cid=None, name=None):
    params = dict(vmem_limit_bytes=60 * 1024 * 1024)
    if cid is not None:
        params.update(collective_id=cid, has_side_effects=True)

    def call(*args):
        specs = [
            pl.BlockSpec(memory_space=pltpu.SMEM if k < smem else VMEM) for k in range(len(args))
        ]
        return pl.pallas_call(
            body,
            out_shape=tuple(jax.ShapeDtypeStruct(s, d) for s, d in outs),
            in_specs=specs,
            out_specs=tuple(pl.BlockSpec(memory_space=VMEM) for _ in outs),
            scratch_shapes=list(scratch),
            compiler_params=pltpu.CompilerParams(**params),
            name=name,
        )(*args)

    return call


def places(nz, ny):
    z, y, t = lax.axis_index("z"), lax.axis_index("y"), lax.axis_index("tp")

    def at(dz, dy):
        return (lax.rem(z + (dz + nz), nz), lax.rem(y + (dy + ny), ny), t)

    return z, y, at


def remote(src, dst, ssem, rsem, device):
    return pltpu.make_async_remote_copy(
        src_ref=src, dst_ref=dst, send_sem=ssem, recv_sem=rsem, device_id=device, device_id_type=MESH
    )


def meet(peers):
    barrier = pltpu.get_barrier_semaphore()
    for peer in peers:
        pl.semaphore_signal(barrier, inc=1, device_id=peer, device_id_type=MESH)
    pl.semaphore_wait(barrier, len(peers))


class Link:
    def __init__(self, sems, own):
        self.sems, self.own, self.sent = sems, own, []

    def start(self, step, src, dst, device):
        copy = remote(src, dst, self.sems.at[0, step], self.sems.at[1, step], device)
        copy.start()
        self.sent.append(copy)

    def arrived(self, step, dst):
        remote(dst, dst, self.sems.at[0, step], self.sems.at[1, step], self.own).wait_recv()

    def drain(self):
        for copy in self.sent:
            copy.wait_send()


def weights_kernel(nz, ny, wa, wb, oa, ob, local, ya, za_up, za_dn, zb_up, zb_dn, y_up, y_dn, y_far):
    z, y, at = places(nz, ny)
    up, down, left, right = at(1, 0), at(-1, 0), at(0, -1), at(0, 1)
    meet([up, down, left, right, at(0, 2)])
    row = lambda d: lax.rem(z + (d + nz), nz)
    col = lambda d: lax.rem(y + (d + ny), ny)
    ups, dns = nz // 2, nz // 2 - 1
    links = [Link(s, up) for s in (ya, za_up, za_dn, zb_up, zb_dn, y_up, y_dn, y_far)]
    ya, za_up, za_dn, zb_up, zb_dn, y_up, y_dn, y_far = links
    keep_a = pltpu.make_async_copy(wa, oa.at[z, y], local.at[0])
    keep_b = pltpu.make_async_copy(wb, ob.at[z, y], local.at[1])
    keep_a.start()
    keep_b.start()
    for d in (1, 3, 2):
        ya.start(d - 1, wa, oa.at[z, y], at(0, d))
    zb_up.start(0, wb, ob.at[z, y], up)
    zb_dn.start(0, wb, ob.at[z, y], down)

    def fan(k, zz, src):
        y_up.start(k, src, ob.at[zz, y], right)
        y_dn.start(k, src, ob.at[zz, y], left)

    def far(k, zz):
        y_up.arrived(k, ob.at[zz, col(-1)])
        y_dn.arrived(k, ob.at[zz, col(1)])
        if k % 2 == 0:
            y_far.start(k, ob.at[zz, col(-1)], ob.at[zz, col(-1)], right)
        else:
            y_far.start(k, ob.at[zz, col(1)], ob.at[zz, col(1)], left)

    fan(0, z, wb)
    for d in (1, 3, 2):
        ya.arrived(d - 1, oa.at[z, col(-d)])
    keep_a.wait()
    za_up.start(0, oa.at[z], oa.at[z], up)
    za_dn.start(0, oa.at[z], oa.at[z], down)
    waiting = [(0, z)]
    for s in range(ups):
        fresh = []
        for sign, steps, zb, za, to in ((-1, ups, zb_up, za_up, up), (1, dns, zb_dn, za_dn, down)):
            if s >= steps:
                continue
            zz = row(sign * (s + 1))
            zb.arrived(s, ob.at[zz, y])
            if s + 1 < steps:
                zb.start(s + 1, ob.at[zz, y], ob.at[zz, y], to)
            k = 2 * s + (1 if sign < 0 else 2)
            fan(k, zz, ob.at[zz, y])
            fresh.append((k, zz))
            za.arrived(s, oa.at[zz])
            if s + 1 < steps:
                za.start(s + 1, oa.at[zz], oa.at[zz], to)
        for k, zz in waiting:
            far(k, zz)
        waiting = fresh
    for k, zz in waiting:
        far(k, zz)
    for k in range(nz):
        y_far.arrived(k, ob.at[row(0), col(2)])
    keep_b.wait()
    for link in links:
        link.drain()


def gather_weights(nz, ny, wa, wb):
    sems = lambda n: pltpu.SemaphoreType.DMA((2, n))
    ups, dns = nz // 2, nz // 2 - 1
    return vmem_call(
        functools.partial(weights_kernel, nz, ny),
        [((nz, ny) + wa.shape, wa.dtype), ((nz, ny) + wb.shape, wb.dtype)],
        [pltpu.SemaphoreType.DMA((2,)), sems(ny - 1)]
        + [sems(ups), sems(dns)] * 2
        + [sems(nz)] * 3,
        cid=1,
        name="gather_weights",
    )(wa, wb)


def exchange_kernel(nz, ny, n_ring, n_all, n_swap, *refs):
    n = n_ring + n_all + n_swap
    ins, outs, sems = refs[:n], refs[n : 2 * n], refs[2 * n :]
    local, sems = sems[0], sems[1:]
    z, y, at = places(nz, ny)
    up, down = at(1, 0), at(-1, 0)
    row = lambda d: lax.rem(z + (d + nz), nz)
    col = lambda d: lax.rem(y + (d + ny), ny)
    ups, dns = nz // 2, nz // 2 - 1
    peers = [up, down] if n_ring else []
    if n_all + n_swap:
        peers += [at(0, d) for d in range(1, ny)]
    meet(peers)
    links, keeps, rings, flats = [], [], [], []
    for k in range(n):
        src, dst = ins[k], outs[k]
        if k < n_ring:
            up_link, dn_link = Link(sems[0], up), Link(sems[1], up)
            sems = sems[2:]
            up_link.start(0, src, dst.at[z], up)
            dn_link.start(0, src, dst.at[z], down)
            rings.append((dst, up_link, dn_link))
            links += [up_link, dn_link]
            keep = pltpu.make_async_copy(src, dst.at[z], local.at[k])
        else:
            link, sems = Link(sems[0], up), sems[1:]
            swap = k >= n_ring + n_all
            for d in (1, 3, 2):
                link.start(d - 1, src.at[col(d)] if swap else src, dst.at[y], at(0, d))
            flats.append((dst, link))
            links.append(link)
            keep = pltpu.make_async_copy(src.at[y] if swap else src, dst.at[y], local.at[k])
        keep.start()
        keeps.append(keep)
    if n_ring:
        for s in range(ups):
            for dst, up_link, dn_link in rings:
                for sign, steps, link, to in ((-1, ups, up_link, up), (1, dns, dn_link, down)):
                    if s >= steps:
                        continue
                    zz = row(sign * (s + 1))
                    link.arrived(s, dst.at[zz])
                    if s + 1 < steps:
                        link.start(s + 1, dst.at[zz], dst.at[zz], to)
    for dst, link in flats:
        for d in (1, 3, 2):
            link.arrived(d - 1, dst.at[col(-d)])
    for keep in keeps:
        keep.wait()
    for link in links:
        link.drain()


def exchange(nz, ny, cid, name, ring=(), all_y=(), swap_y=()):
    sems = lambda n: pltpu.SemaphoreType.DMA((2, n))
    outs = [((nz,) + a.shape, a.dtype) for a in ring]
    outs += [((ny,) + a.shape, a.dtype) for a in all_y]
    outs += [(a.shape, a.dtype) for a in swap_y]
    scratch = [pltpu.SemaphoreType.DMA((len(outs),))]
    for _ in ring:
        scratch += [sems(nz // 2), sems(nz // 2 - 1)]
    scratch += [sems(ny - 1)] * (len(all_y) + len(swap_y))
    return vmem_call(
        functools.partial(exchange_kernel, nz, ny, len(ring), len(all_y), len(swap_y)),
        outs,
        scratch,
        cid=cid,
        name=name,
    )(*ring, *all_y, *swap_y)


def iotas(shape):
    return lax.broadcasted_iota(jnp.int32, shape, 0), lax.broadcasted_iota(jnp.int32, shape, 1)


def softplus(x):
    return jnp.maximum(x, 0.0) + jnp.log1p(jnp.exp(-jnp.abs(x)))


def sigmoid(x):
    return 1.0 / (1.0 + jnp.exp(-x))


def unit_rows(values):
    return values * lax.rsqrt(jnp.sum(jnp.square(values), axis=-1, keepdims=True) + 1e-06)


def project_kernel(
    place, tok, gain, oa, ob, wbd, vec, extra, qt, kv, mb, solved_ref, qk_ref, qd_ref
):
    t = place[2]
    values = tok[...].astype(F32)
    center = jnp.mean(values, axis=-1, keepdims=True)
    shifted = values - center
    spread = jnp.mean(jnp.square(shifted), axis=-1, keepdims=True)
    normed = (shifted * lax.rsqrt(spread + 1e-05) * gain[...]).astype(BF16)
    attn = dot(normed, oa[...]).astype(BF16)
    delta = dot(normed, ob[:, : 3 * 128]).astype(BF16).astype(F32)
    gates = dot(normed, wbd[...]).astype(BF16).astype(F32)
    qt[...] = jnp.transpose(attn[:, :128].astype(F32)).astype(BF16)
    r, c = iotas((ROWS, ROWS))
    shuffle = jnp.where(c == (r & 7) * (ROWS // 8) + (r >> 3), 1.0, 0.0).astype(BF16)
    kv[0] = dot(shuffle, attn[:, 128:256]).astype(BF16)
    kv[1] = dot(shuffle, attn[:, 256:384]).astype(BF16)

    n_gate = wbd.shape[1] // 2
    lane = lax.broadcasted_iota(jnp.int32, (1, 2 * n_gate), 1)

    def pick(a, where):
        return jnp.sum(jnp.where(lane == where, a, 0.0), axis=-1, keepdims=True)

    beta = sigmoid(pick(gates, t) + pick(vec[...], t))
    rate = jnp.exp(pick(vec[...], n_gate + t))
    decay = -rate * softplus(pick(gates, n_gate + t)) + extra[...]
    silu = delta * sigmoid(delta)
    queries = unit_rows(silu[:, :128]) * (128.0**-0.5)
    keys = unit_rows(silu[:, 128:256])
    vals = silu[:, 256:]
    lower = r >= c
    total = exact(jnp.where(lower, 1.0, 0.0), jnp.broadcast_to(decay, (ROWS, 128)))
    across = jnp.transpose(total)[:1, :]
    total = total[:, :1]
    end = total[ROWS - 1 :, :]
    mask = jnp.where(lower, jnp.exp(jnp.where(lower, total - across, 0.0)), 0.0)
    keys_beta = keys * beta
    grown = jnp.exp(total)
    nmat = jnp.where(r > c, exact(keys_beta, keys, ((1,), (1,))) * mask, 0.0)
    near = jnp.where((r >> 3) == (c >> 3), nmat, 0.0)
    two = exact(near, near)
    four = exact(two, two)
    inv = jnp.where(r == c, 1.0, 0.0) - near
    inv = inv + exact(inv, two)
    inv = inv + exact(inv, four)
    for bit in range(3, 8):
        cross = ((r >> (bit + 1)) == (c >> (bit + 1))) & ((r >> bit) != (c >> bit))
        part = jnp.where(cross, nmat, 0.0)
        inv = inv - exact(inv, exact(part, inv))
    solved = exact(inv, jnp.concatenate([keys_beta * grown, vals * beta], axis=1))
    solved_ref[...] = solved
    qk_ref[...] = exact(queries, keys, ((1,), (1,))) * mask
    qd_ref[...] = queries * grown
    to_end = keys * jnp.exp(end - total)
    written = exact(to_end, solved, ((0,), (0,)))
    rr, cc = iotas((128, 256))
    mb[...] = jnp.where(cc < 128, jnp.where(rr == cc, jnp.exp(end), 0.0) - written, written)


def attend_kernel(place, bias, kv, qt, mbs, o_ref, l_ref, total_ref, before_ref):
    z, y = place[0], place[1]
    nz, ny = kv.shape[0], qt.shape[0]
    groups = ROWS // 8
    sub = lax.broadcasted_iota(jnp.int32, (8, ROWS), 0)
    query = lax.broadcasted_iota(jnp.int32, (8, ROWS), 1)

    def tile(zp, yq, masked):
        sums = []
        for h in range(2):
            scores = dot(kv[zp, 0, :, h * 64 : h * 64 + 64], qt[yq, h * 64 : h * 64 + 64, :])
            run = jnp.zeros((8, ROWS), F32)
            left = [None] * groups
            for g in reversed(range(groups)):
                u = scores[g * 8 : g * 8 + 8] * (0.125 * LOG2E) + bias[0, h] * LOG2E
                lost = jnp.maximum(u, jnp.log2(1.0 + jnp.exp2(jnp.minimum(u, 100.0))))
                if masked:
                    lost = jnp.where(sub * groups + g < query + ROWS * (yq - y), lost, 0.0)
                run = run + lost
                left[g] = u - run
            incl = run
            for d in (1, 2, 4):
                incl = incl + jnp.where(sub < 8 - d, pltpu.roll(incl, 8 - d, 0), 0.0)
            later = jnp.where(sub < 7, pltpu.roll(incl, 7, 0), 0.0)
            weights = []
            for g in range(groups):
                w = jnp.exp2(left[g] - later)
                if masked:
                    w = jnp.where(sub * groups + g < query + ROWS * (yq - y), w, 0.0)
                weights.append(w)
            weights = jnp.concatenate(weights, axis=0).astype(BF16)
            o_ref[zp, yq, h * 64 : h * 64 + 64, :] = dot(
                kv[zp, 1, :, h * 64 : h * 64 + 64], weights, ((0,), (0,))
            )
            sums.append(incl[:1])
        l_ref[zp, yq] = jnp.concatenate(sums, axis=0)

    l_ref[...] = jnp.zeros_like(l_ref)

    @pl.loop(0, z * ny)
    def _(k):
        tile(lax.div(k, ny), lax.rem(k, ny), False)

    @pl.loop(0, ny)
    def _(yq):
        tile(z, yq, True)

    rr, cc = iotas((128, 256))
    chain = jnp.where(rr == cc, 1.0, 0.0)
    before = chain
    for k in range(ny):
        m = mbs[k]
        before = jnp.where(y == k, chain, before)
        chain = exact(m[:, :128], chain) + jnp.where(cc < 128, 0.0, m)
    before_ref[...] = before
    total_ref[...] = chain


def combine_kernel(
    place, o_ref, l_ref, totals, before, solved, qk, qd, gain, part_ref, delta_ref, state
):
    z, y = place[0], place[1]
    ny = l_ref.shape[0]
    part_ref[...] = jnp.zeros_like(part_ref)

    def one(i, later):
        zp = z - i
        sums = [l_ref[k, zp] for k in range(ny)]
        here = later
        for k in range(ny):
            here = here + jnp.where(k > y, sums[k], 0.0)
            later = later + sums[k]
        kept = jnp.exp2(-here)
        for yq in range(ny):
            for h in range(2):
                rows = slice(h * 64, h * 64 + 64)
                part_ref[yq, rows, :] += o_ref[zp, yq, rows, :] * kept[yq, h : h + 1, :]
        return later

    lax.fori_loop(0, z + 1, one, jnp.zeros(l_ref.shape[2:], F32))
    state[...] = jnp.zeros_like(state)

    @pl.loop(0, z)
    def _(k):
        state[...] = exact(totals[k, :, :128], state[...]) + totals[k, :, 128:]

    incoming = exact(before[:, :128], state[...]) + before[:, 128:]
    fresh = solved[:, 128:] - exact(solved[:, :128], incoming)
    raw = exact(qd[...], incoming) + exact(qk[...], fresh)
    scale = lax.rsqrt(jnp.mean(jnp.square(raw), axis=-1, keepdims=True) + 1e-06)
    delta_ref[...] = (raw * scale * gain[...]).astype(BF16)


def output_kernel(parts, delta, gain, wo, out):
    raw = parts[0]
    for k in range(1, parts.shape[0]):
        raw = raw + parts[k]
    halves = []
    for h in range(2):
        half = raw[h * 64 : h * 64 + 64]
        halves.append(half * lax.rsqrt(jnp.mean(jnp.square(half), axis=0, keepdims=True) + 1e-06))
    attn = (jnp.transpose(jnp.concatenate(halves, axis=0)) * gain[...]).astype(BF16)
    mixed = jnp.concatenate([attn, delta[...]], axis=1)
    out[...] = dot(mixed, wo[...], ((1,), (1,))).astype(BF16)


def local(
    nz,
    ny,
    tokens,
    ln_gain,
    w_query_attn,
    w_key_attn,
    w_value_attn,
    w_query_delta,
    w_key_delta,
    w_value_delta,
    w_beta,
    w_decay,
    attn_bias,
    decay_log,
    beta_bias,
    log_decay_extra,
    attn_gain,
    delta_gain,
    w_out_attn,
    w_out_delta,
):
    z, y, t = lax.axis_index("z"), lax.axis_index("y"), lax.axis_index("tp")
    place = jnp.stack([z, y, t]).astype(jnp.int32)
    wa = jnp.concatenate([w_query_attn, w_key_attn, w_value_attn], axis=1)
    wb = jnp.concatenate(
        [w_query_delta, w_key_delta, w_value_delta, w_out_attn.T, w_out_delta.T], axis=1
    )
    oa, ob = gather_weights(nz, ny, wa, wb)
    oa = oa.reshape(-1, oa.shape[-1])
    ob = ob.reshape(-1, ob.shape[-1])
    wbd = jnp.concatenate([w_beta, w_decay], axis=1)
    vec = jnp.concatenate([beta_bias, decay_log])[None]
    qt, kv, mb, solved, qk, qd = vmem_call(
        project_kernel,
        [
            ((128, ROWS), BF16),
            ((2, ROWS, 128), BF16),
            ((128, 256), F32),
            ((ROWS, 256), F32),
            ((ROWS, ROWS), F32),
            ((ROWS, 128), F32),
        ],
        smem=1,
        name="project",
    )(place, tokens, ln_gain[None], oa, ob, wbd, vec, log_decay_extra)
    kvs, qts, mbs = exchange(nz, ny, 2, "gather_keys", ring=(kv,), all_y=(qt, mb))
    bias = lax.dynamic_slice_in_dim(attn_bias, 2 * t, 2, 0)[None]
    o, sums, total, before = vmem_call(
        attend_kernel,
        [
            ((nz, ny, 128, ROWS), F32),
            ((nz, ny, 2, ROWS), F32),
            ((128, 256), F32),
            ((128, 256), F32),
        ],
        smem=2,
        name="attend",
    )(place, bias, kvs, qts, mbs)
    totals, all_sums = exchange(nz, ny, 3, "gather_states", ring=(total,), all_y=(sums,))
    parts, delta = vmem_call(
        combine_kernel,
        [((ny, 128, ROWS), F32), ((ROWS, 128), BF16)],
        [pltpu.VMEM((128, 128), F32)],
        smem=1,
        name="combine",
    )(place, o, all_sums, totals, before, solved, qk, qd, delta_gain[None])
    (parts,) = exchange(nz, ny, 4, "swap_parts", swap_y=(parts,))
    gain2 = jnp.concatenate([attn_gain, attn_gain])[None]
    (partial,) = vmem_call(output_kernel, [((ROWS, ob.shape[0]), BF16)], name="output")(
        parts, delta, gain2, ob[:, 3 * 128 :]
    )
    n_tp = lax.axis_size("tp")
    pieces = partial.reshape(n_tp, ROWS // n_tp, -1)
    pieces = lax.all_to_all(pieces, "tp", 0, 0, tiled=True)
    return jnp.sum(pieces.astype(F32), axis=0).astype(BF16)


def solution(mesh):
    nz, ny = 16, 4
    split = Mesh(mesh.devices.reshape(nz, ny, mesh.shape["tp"]), ("z", "y", "tp"))
    return jax.shard_map(
        functools.partial(local, nz, ny),
        mesh=split,
        in_specs=(
            P(SP, None),
            P(),
            P(SP, "tp"),
            P(SP, "tp"),
            P(SP, "tp"),
            P(SP, "tp"),
            P(SP, "tp"),
            P(SP, "tp"),
            P(),
            P(),
            P(),
            P(),
            P(),
            P(SP, "tp"),
            P(),
            P(),
            P("tp", SP),
            P("tp", SP),
        ),
        out_specs=P(SP + ("tp",), None),
        check_vma=False,
    )
```

```python
import functools

import jax
import jax.numpy as jnp
from jax import lax
from jax.experimental import pallas as pl
from jax.experimental.pallas import tpu as pltpu
from jax.sharding import Mesh
from jax.sharding import PartitionSpec as P

MESH = pl.DeviceIdType.MESH
VMEM = pltpu.VMEM
SP = ("z", "y")
LOG2E = 1.4426950408889634
ROWS = 256
F32 = jnp.float32
BF16 = jnp.bfloat16
HIGH = lax.Precision.HIGHEST


def dot(a, b, dims=((1,), (0,)), precision=None):
    return lax.dot_general(
        a, b, (dims, ((), ())), precision=precision, preferred_element_type=F32
    )


def exact(a, b, dims=((1,), (0,))):
    return dot(a, b, dims, HIGH)


def split(a):
    high = a.astype(BF16)
    return high, (a - high.astype(F32)).astype(BF16)


def close(a, b, dims=((1,), (0,))):
    (ah, al), (bh, bl) = split(a), split(b)
    return dot(ah, bh, dims) + (dot(ah, bl, dims) + dot(al, bh, dims))


def apply_rounded(a, b):
    high, low = split(b)
    return dot(a, high) + dot(a, low)


def vmem_call(body, outs, scratch=(), smem=0, cid=None, name=None):
    params = dict(vmem_limit_bytes=60 * 1024 * 1024)
    if cid is not None:
        params.update(collective_id=cid, has_side_effects=True)

    def call(*args):
        specs = [
            pl.BlockSpec(memory_space=pltpu.SMEM if k < smem else VMEM) for k in range(len(args))
        ]
        return pl.pallas_call(
            body,
            out_shape=tuple(jax.ShapeDtypeStruct(s, d) for s, d in outs),
            in_specs=specs,
            out_specs=tuple(pl.BlockSpec(memory_space=VMEM) for _ in outs),
            scratch_shapes=list(scratch),
            compiler_params=pltpu.CompilerParams(**params),
            name=name,
        )(*args)

    return call


def places(nz, ny):
    z, y, t = lax.axis_index("z"), lax.axis_index("y"), lax.axis_index("tp")

    def at(dz, dy):
        return (lax.rem(z + (dz + nz), nz), lax.rem(y + (dy + ny), ny), t)

    return z, y, at


def remote(src, dst, ssem, rsem, device):
    return pltpu.make_async_remote_copy(
        src_ref=src, dst_ref=dst, send_sem=ssem, recv_sem=rsem, device_id=device, device_id_type=MESH
    )


def meet(peers):
    barrier = pltpu.get_barrier_semaphore()
    for peer in peers:
        pl.semaphore_signal(barrier, inc=1, device_id=peer, device_id_type=MESH)
    pl.semaphore_wait(barrier, len(peers))


class Link:
    def __init__(self, sems, own):
        self.sems, self.own, self.sent = sems, own, []

    def start(self, step, src, dst, device):
        copy = remote(src, dst, self.sems.at[0, step], self.sems.at[1, step], device)
        copy.start()
        self.sent.append(copy)

    def arrived(self, step, dst):
        remote(dst, dst, self.sems.at[0, step], self.sems.at[1, step], self.own).wait_recv()

    def drain(self):
        for copy in self.sent:
            copy.wait_send()


def weights_kernel(nz, ny, n_a, n_b, *refs):
    n = n_a + n_b
    ins, (oa, ob) = refs[:n], refs[n : n + 2]
    local, ya, za_up, za_dn, zb_up, zb_dn, y_up, y_dn, y_far = refs[n + 2 :]
    z, y, at = places(nz, ny)
    up, down, left, right = at(1, 0), at(-1, 0), at(0, -1), at(0, 1)
    row = lambda d: lax.rem(z + (d + nz), nz)
    col = lambda d: lax.rem(y + (d + ny), ny)
    ups, dns = nz // 2, nz // 2 - 1
    links = [Link(s, up) for s in (ya, za_up, za_dn, zb_up, zb_dn, y_up, y_dn, y_far)]
    ya, za_up, za_dn, zb_up, zb_dn, y_up, y_dn, y_far = links
    packs = []
    for k in range(n):
        out, place = (oa, k) if k < n_a else (ob, k - n_a)
        dst = out.at[z, y, :, pl.ds(128 * place, 128)]
        packs.append(pltpu.make_async_copy(ins[k], dst, local.at[k]))
        packs[-1].start()
    meet([up, down, left, right, at(0, 2)])
    for pack in packs:
        pack.wait()
    order = (0, 3, 1, 2)
    for d in (1, 3, 2):
        ya.start(d - 1, oa.at[z, y], oa.at[z, y], at(0, d))

    def lead(c):
        block = oa.at[z, col(c)]
        za_up.start(c, block, block, up)
        za_dn.start(c, block, block, down)

    def fan(k, zz):
        y_up.start(k, ob.at[zz, y], ob.at[zz, y], right)
        y_dn.start(k, ob.at[zz, y], ob.at[zz, y], left)

    def far(k, zz):
        y_up.arrived(k, ob.at[zz, col(-1)])
        y_dn.arrived(k, ob.at[zz, col(1)])
        if k % 2 == 0:
            y_far.start(k, ob.at[zz, col(-1)], ob.at[zz, col(-1)], right)
        else:
            y_far.start(k, ob.at[zz, col(1)], ob.at[zz, col(1)], left)

    lead(0)
    zb_up.start(0, ob.at[z, y], ob.at[z, y], up)
    zb_dn.start(0, ob.at[z, y], ob.at[z, y], down)
    fan(0, z)
    for c in order[1:]:
        ya.arrived(ny - c - 1, oa.at[z, col(c)])
        lead(c)
    waiting = [(0, z)]
    ways = ((-1, ups, zb_up, za_up, up), (1, dns, zb_dn, za_dn, down))
    for s in range(ups):
        fresh = []
        for c in order:
            for sign, steps, zb, za, to in ways:
                if s >= steps:
                    continue
                zz = row(sign * (s + 1))
                za.arrived(s * ny + c, oa.at[zz, col(c)])
                if s + 1 < steps:
                    za.start((s + 1) * ny + c, oa.at[zz, col(c)], oa.at[zz, col(c)], to)
                if c == 0:
                    zb.arrived(s, ob.at[zz, y])
                    if s + 1 < steps:
                        zb.start(s + 1, ob.at[zz, y], ob.at[zz, y], to)
                    k = 2 * s + (1 if sign < 0 else 2)
                    fan(k, zz)
                    fresh.append((k, zz))
        for k, zz in waiting:
            far(k, zz)
        waiting = fresh
    for k, zz in waiting:
        far(k, zz)
    for k in range(nz):
        y_far.arrived(k, ob.at[z, col(2)])
    for link in links:
        link.drain()


def gather_weights(nz, ny, set_a, set_b):
    sems = lambda n: pltpu.SemaphoreType.DMA((2, n))
    ups, dns = nz // 2, nz // 2 - 1
    n_a, n_b = len(set_a), len(set_b)
    rows, dtype = set_a[0].shape[0], set_a[0].dtype
    return vmem_call(
        functools.partial(weights_kernel, nz, ny, n_a, n_b),
        [((nz, ny, rows, 128 * n_a), dtype), ((nz, ny, rows, 128 * n_b), dtype)],
        [pltpu.SemaphoreType.DMA((n_a + n_b,)), sems(ny - 1), sems(ups * ny), sems(dns * ny)]
        + [sems(ups), sems(dns)]
        + [sems(nz)] * 3,
        cid=1,
        name="gather_weights",
    )(*set_a, *set_b)


def identity_part():
    rr, cc = iotas((128, 256))
    return jnp.where(rr == cc, 1.0, 0.0), cc < 128


def keys_kernel(nz, ny, *refs):
    kv, qt, mb, kvs, qts, mbs, totals, before = refs[:8]
    local, y_q, y_m, k_up, k_dn, t_up, t_dn = refs[8:]
    z, y, at = places(nz, ny)
    up, down = at(1, 0), at(-1, 0)
    row = lambda d: lax.rem(z + (d + nz), nz)
    col = lambda d: lax.rem(y + (d + ny), ny)
    ups, dns = nz // 2, nz // 2 - 1
    links = [Link(s, up) for s in (y_q, y_m, k_up, k_dn, t_up, t_dn)]
    y_q, y_m, k_up, k_dn, t_up, t_dn = links
    meet([up, down] + [at(0, d) for d in range(1, ny)])
    keeps = [
        pltpu.make_async_copy(kv, kvs.at[z], local.at[0]),
        pltpu.make_async_copy(qt, qts.at[y], local.at[1]),
        pltpu.make_async_copy(mb, mbs.at[y], local.at[2]),
    ]
    for d in (1, 3, 2):
        y_m.start(d - 1, mb, mbs.at[y], at(0, d))
    half = kv.shape[1] // 2
    part = lambda ref, p: ref.at[p // 2, pl.ds(half * (p % 2), half)]
    for p in range(4):
        k_up.start(p, part(kv, p), part(kvs.at[z], p), up)
        k_dn.start(p, part(kv, p), part(kvs.at[z], p), down)
    for d in (1, 3, 2):
        y_q.start(d - 1, qt, qts.at[y], at(0, d))
    for keep in keeps:
        keep.start()
    ways = ((-1, ups, k_up, t_up, up), (1, dns, k_dn, t_dn, down))
    t_rows = totals.shape[1] // 2
    piece = lambda zz, p: totals.at[zz, pl.ds(t_rows * p, t_rows)]
    lag = 2
    for s in range(ups + lag):
        for sign, steps, link, _, to in ways:
            if s < steps:
                zz = row(sign * (s + 1))
                for p in range(4):
                    block = part(kvs.at[zz], p)
                    link.arrived(4 * s + p, block)
                    if s + 1 < steps:
                        link.start(4 * (s + 1) + p, block, block, to)
        if s == 0:
            for d in (1, 3, 2):
                y_m.arrived(d - 1, mbs.at[col(-d)])
            keeps[2].wait()
            eye, left_half = identity_part()
            chain, first = eye, eye
            for k in range(ny):
                m = mbs[k]
                first = jnp.where(y == k, chain, first)
                shift = chain + jnp.where(left_half, 0.0, m.astype(F32))
                chain = apply_rounded(m[:, :128], chain) + shift
            before[...] = first
            totals[z] = (chain - eye).astype(BF16)
        if s == lag - 1:
            for p in range(2):
                t_up.start(p, piece(z, p), piece(z, p), up)
                t_dn.start(p, piece(z, p), piece(z, p), down)
        if s >= lag:
            for sign, steps, _, link, to in ways:
                if s - lag < steps:
                    zz = row(sign * (s - lag + 1))
                    for p in range(2):
                        link.arrived(2 * (s - lag) + p, piece(zz, p))
                        if s - lag + 1 < steps:
                            link.start(2 * (s - lag + 1) + p, piece(zz, p), piece(zz, p), to)
    for d in (1, 3, 2):
        y_q.arrived(d - 1, qts.at[col(-d)])
    keeps[0].wait()
    keeps[1].wait()
    for link in links:
        link.drain()


def gather_keys(nz, ny, kv, qt, mb):
    sems = lambda n: pltpu.SemaphoreType.DMA((2, n))
    ups, dns = nz // 2, nz // 2 - 1
    return vmem_call(
        functools.partial(keys_kernel, nz, ny),
        [
            ((nz,) + kv.shape, kv.dtype),
            ((ny,) + qt.shape, qt.dtype),
            ((ny,) + mb.shape, mb.dtype),
            ((nz,) + mb.shape, BF16),
            (mb.shape, F32),
        ],
        [pltpu.SemaphoreType.DMA((3,)), sems(ny - 1), sems(ny - 1)]
        + [sems(4 * ups), sems(4 * dns), sems(2 * ups), sems(2 * dns)],
        cid=2,
        name="gather_keys",
    )(kv, qt, mb)


def sums_kernel(ny, sums, every, local, y_s):
    _, y, at = places(1, ny)
    z = lax.axis_index("z")
    t = lax.axis_index("tp")
    col = lambda d: lax.rem(y + (d + ny), ny)
    peer = lambda d: (z, col(d), t)
    link = Link(y_s, peer(1))
    meet([peer(d) for d in range(1, ny)])
    for d in (1, 3, 2):
        link.start(d - 1, sums, every.at[y], peer(d))
    keep = pltpu.make_async_copy(sums, every.at[y], local.at[0])
    keep.start()
    for d in (1, 3, 2):
        link.arrived(d - 1, every.at[col(-d)])
    keep.wait()
    link.drain()


def gather_sums(ny, sums):
    return vmem_call(
        functools.partial(sums_kernel, ny),
        [((ny,) + sums.shape, sums.dtype)],
        [pltpu.SemaphoreType.DMA((1,)), pltpu.SemaphoreType.DMA((2, ny - 1))],
        cid=3,
        name="gather_sums",
    )(sums)[0]


def iotas(shape):
    return lax.broadcasted_iota(jnp.int32, shape, 0), lax.broadcasted_iota(jnp.int32, shape, 1)


def softplus(x):
    return jnp.maximum(x, 0.0) + jnp.log1p(jnp.exp(-jnp.abs(x)))


def sigmoid(x):
    return 1.0 / (1.0 + jnp.exp(-x))


def unit_rows(values):
    return values * lax.rsqrt(jnp.sum(jnp.square(values), axis=-1, keepdims=True) + 1e-06)


def project_kernel(
    place,
    tok,
    gain,
    oa,
    ob,
    w_beta,
    w_decay,
    beta_bias,
    decay_log,
    extra,
    qt,
    kv,
    mb,
    solved_ref,
    qk_ref,
    qd_ref,
):
    t = place[2]
    values = tok[...].astype(F32)
    center = jnp.mean(values, axis=-1, keepdims=True)
    shifted = values - center
    spread = jnp.mean(jnp.square(shifted), axis=-1, keepdims=True)
    normed = (shifted * lax.rsqrt(spread + 1e-05) * gain[...]).astype(BF16)
    attn = dot(normed, oa[...]).astype(BF16)
    delta = dot(normed, ob[:, : 3 * 128]).astype(BF16).astype(F32)
    beta_pre = dot(normed, w_beta[...], ((1,), (1,))).astype(BF16).astype(F32)
    decay_pre = dot(normed, w_decay[...], ((1,), (1,))).astype(BF16).astype(F32)
    qt[...] = jnp.transpose(attn[:, :128].astype(F32)).astype(BF16)
    r, c = iotas((ROWS, ROWS))
    shuffle = jnp.where(c == (r & 7) * (ROWS // 8) + (r >> 3), 1.0, 0.0).astype(BF16)
    kv[0] = dot(shuffle, attn[:, 128:256]).astype(BF16)
    kv[1] = dot(shuffle, attn[:, 256:384]).astype(BF16)

    lane = lax.broadcasted_iota(jnp.int32, (1, w_beta.shape[0]), 1)

    def pick(a):
        return jnp.sum(jnp.where(lane == t, a, 0.0), axis=-1, keepdims=True)

    beta = sigmoid(pick(beta_pre) + pick(beta_bias[...]))
    rate = jnp.exp(pick(decay_log[...]))
    added = jnp.transpose(jnp.broadcast_to(extra[...], (8, ROWS)))[:, :1]
    decay = -rate * softplus(pick(decay_pre)) + added
    silu = delta * sigmoid(delta)
    queries = unit_rows(silu[:, :128]) * (128.0**-0.5)
    keys = unit_rows(silu[:, 128:256])
    vals = silu[:, 256:]
    lower = r >= c
    total = exact(jnp.where(lower, 1.0, 0.0), jnp.broadcast_to(decay, (ROWS, 128)))
    across = jnp.transpose(total)[:1, :]
    total = total[:, :1]
    end = total[ROWS - 1 :, :]
    mask = jnp.where(lower, jnp.exp(jnp.where(lower, total - across, 0.0)), 0.0)
    keys_beta = keys * beta
    grown = jnp.exp(total)
    nmat = jnp.where(r > c, close(keys_beta, keys, ((1,), (1,))) * mask, 0.0)
    near = jnp.where((r >> 3) == (c >> 3), nmat, 0.0)
    two = close(near, near)
    four = close(two, two)
    inv = jnp.where(r == c, 1.0, 0.0) - near
    inv = inv + close(inv, two)
    inv = inv + close(inv, four)
    for bit in range(3, 8):
        cross = ((r >> (bit + 1)) == (c >> (bit + 1))) & ((r >> bit) != (c >> bit))
        part = jnp.where(cross, nmat, 0.0)
        inv = inv - close(inv, close(part, inv))
    solved = close(inv, jnp.concatenate([keys_beta * grown, vals * beta], axis=1))
    solved_ref[...] = solved
    qk_ref[...] = close(queries, keys, ((1,), (1,))) * mask
    qd_ref[...] = queries * grown
    to_end = keys * jnp.exp(end - total)
    written = close(to_end, solved, ((0,), (0,)))
    eye, left_half = identity_part()
    mb[...] = jnp.where(left_half, eye * (jnp.exp(end) - 1.0) - written, written).astype(BF16)


def attend_kernel(place, bias, kv, qt, o_ref, l_ref, s_even, s_odd, w_even, w_odd):
    z, y = place[0], place[1]
    ny = qt.shape[0]
    groups = ROWS // 8
    sub = lax.broadcasted_iota(jnp.int32, (8, ROWS), 0)
    query = lax.broadcasted_iota(jnp.int32, (8, ROWS), 1)

    def score(k, s):
        zp, yq = lax.div(k, ny), lax.rem(k, ny)
        for h in range(2):
            s[h] = dot(kv[zp, 0, :, h * 64 : h * 64 + 64], qt[yq, h * 64 : h * 64 + 64, :])

    def weigh(k, s, w, masked):
        zp, yq = lax.div(k, ny), lax.rem(k, ny)
        ahead = query + ROWS * (yq - y)
        sums = []
        for h in range(2):
            run = jnp.zeros((8, ROWS), F32)
            left = [None] * groups
            for g in reversed(range(groups)):
                u = s[h, g * 8 : g * 8 + 8, :] * (0.125 * LOG2E) + bias[0, h] * LOG2E
                lost = jnp.maximum(u, jnp.log2(1.0 + jnp.exp2(jnp.minimum(u, 100.0))))
                if masked:
                    lost = jnp.where(sub * groups + g < ahead, lost, 0.0)
                run = run + lost
                left[g] = u - run
            incl = run
            for d in (1, 2, 4):
                incl = incl + jnp.where(sub < 8 - d, pltpu.roll(incl, 8 - d, 0), 0.0)
            later = jnp.where(sub < 7, pltpu.roll(incl, 7, 0), 0.0)
            for g in range(0, groups, 2):
                pair = [jnp.exp2(left[j] - later) for j in (g, g + 1)]
                if masked:
                    pair = [
                        jnp.where(sub * groups + j < ahead, e, 0.0) for e, j in zip(pair, (g, g + 1))
                    ]
                w[h, g * 8 : g * 8 + 16, :] = jnp.concatenate(pair, axis=0).astype(BF16)
            sums.append(incl[:1])
        l_ref[zp, yq] = jnp.concatenate(sums, axis=0)

    def apply(k, w):
        zp, yq = lax.div(k, ny), lax.rem(k, ny)
        for h in range(2):
            o_ref[zp, yq, h * 64 : h * 64 + 64, :] = dot(
                kv[zp, 1, :, h * 64 : h * 64 + 64], w[h], ((0,), (0,))
            ).astype(o_ref.dtype)

    def sweep(first, last, masked):
        score(first, s_even)
        w_odd[...] = jnp.zeros_like(w_odd)

        @pl.loop(0, lax.div(last - first, 2))
        def _(m):
            k = first + 2 * m
            score(k + 1, s_odd)
            weigh(k, s_even, w_even, masked)
            apply(jnp.maximum(k - 1, first), w_odd)
            score(jnp.minimum(k + 2, last - 1), s_even)
            weigh(k + 1, s_odd, w_odd, masked)
            apply(k, w_even)

        apply(last - 1, w_odd)

    l_ref[...] = jnp.zeros_like(l_ref)

    @pl.when(z > 0)
    def _():
        sweep(0, z * ny, False)

    sweep(z * ny, z * ny + ny, True)


def combine_kernel(
    place, o_ref, l_ref, totals, before, solved, qk, qd, gain, part_ref, delta_ref, state, acc
):
    z, y = place[0], place[1]
    ny = l_ref.shape[0]
    acc[...] = jnp.zeros_like(acc)

    def one(i, later):
        zp = z - i
        sums = [l_ref[k, zp] for k in range(ny)]
        here = later
        for k in range(ny):
            here = here + jnp.where(k > y, sums[k], 0.0)
            later = later + sums[k]
        kept = jnp.exp2(-here)
        for yq in range(ny):
            for h in range(2):
                rows = slice(h * 64, h * 64 + 64)
                acc[yq, rows, :] += o_ref[zp, yq, rows, :].astype(F32) * kept[yq, h : h + 1, :]
        return later

    lax.fori_loop(0, z + 1, one, jnp.zeros(l_ref.shape[2:], F32))
    part_ref[...] = acc[...].astype(BF16)
    state[...] = jnp.zeros_like(state)

    @pl.loop(0, z)
    def _(k):
        now = state[...]
        state[...] = now + apply_rounded(totals[k, :, :128], now) + totals[k, :, 128:].astype(F32)

    incoming = close(before[:, :128], state[...]) + before[:, 128:]
    fresh = solved[:, 128:] - close(solved[:, :128], incoming)
    raw = close(qd[...], incoming) + close(qk[...], fresh)
    scale = lax.rsqrt(jnp.mean(jnp.square(raw), axis=-1, keepdims=True) + 1e-06)
    delta_ref[...] = (raw * scale * gain[...]).astype(BF16)


def finish_kernel(
    ny, n_x, parts, delta, gain, wo, out, got, mixed, mine, other, sum_ref, seen, local, y_p, c_p, x_p
):
    y, z, t = lax.axis_index("y"), lax.axis_index("z"), lax.axis_index("tp")
    x, c = lax.div(t, 2), lax.rem(t, 2)
    col = lambda d: lax.rem(y + (d + ny), ny)
    far = lambda d: lax.rem(x + (d + n_x), n_x)
    in_y = lambda d: (z, col(d), t)
    twin = (z, y, 2 * x + (1 - c))
    in_x = lambda d: (z, y, 2 * far(d) + c)
    y_p, c_p, x_p = Link(y_p, twin), Link(c_p, twin), Link(x_p, twin)
    meet([in_y(d) for d in range(1, ny)] + [twin] + [in_x(d) for d in range(1, n_x)])
    for d in (1, 3, 2):
        y_p.start(d - 1, parts.at[col(d)], got.at[y], in_y(d))
    rows = out.shape[0]
    mixed[:, :, :, 128:] = delta[...].reshape(n_x, 2, rows, 128)
    raw = parts[y].astype(F32)
    for d in (1, 3, 2):
        y_p.arrived(d - 1, got.at[col(-d)])
        raw = raw + got[col(-d)].astype(F32)
    halves = []
    for h in range(2):
        half = raw[h * 64 : h * 64 + 64]
        halves.append(half * lax.rsqrt(jnp.mean(jnp.square(half), axis=0, keepdims=True) + 1e-06))
    gains = jnp.concatenate([gain[...], gain[...]], axis=1)
    attn = (jnp.transpose(jnp.concatenate(halves, axis=0)) * gains).astype(BF16)
    mixed[:, :, :, :128] = attn.reshape(n_x, 2, rows, 128)

    def product(core):
        picked = mixed[:, core].reshape(n_x * rows, 256)
        return dot(picked, wo[:, 3 * 128 :], ((1,), (1,))).astype(BF16).reshape(n_x, rows, -1)

    mine[...] = product(1 - c)
    own = product(c)
    c_p.start(0, mine, other, twin)
    sum_ref[...] = own
    c_p.arrived(0, other)
    for d in (2, 1, 3):
        sum_ref[far(d)] = (sum_ref[far(d)].astype(F32) + other[far(d)].astype(F32)).astype(BF16)
    total = sum_ref[x].astype(F32) + other[x].astype(F32)
    for d in (2, 1, 3):
        x_p.start(d - 1, sum_ref.at[far(d)], seen.at[x], in_x(d))
    for d in (1, 3, 2):
        x_p.arrived(d - 1, seen.at[far(-d)])
        total = total + seen[far(-d)].astype(F32)
    out[...] = total.astype(BF16)
    for link in (y_p, c_p, x_p):
        link.drain()


def finish(ny, n_x, parts, delta, gain, wo):
    rows, wide = ROWS // (2 * n_x), wo.shape[0]
    sems = lambda n: pltpu.SemaphoreType.DMA((2, n))
    big = pltpu.VMEM((n_x, rows, wide), BF16)
    return vmem_call(
        functools.partial(finish_kernel, ny, n_x),
        [((rows, wide), BF16)],
        [
            pltpu.VMEM(parts.shape, parts.dtype),
            pltpu.VMEM((n_x, 2, rows, 256), BF16),
            big,
            big,
            big,
            big,
            pltpu.SemaphoreType.DMA((1,)),
            sems(ny - 1),
            sems(1),
            sems(n_x - 1),
        ],
        cid=4,
        name="finish",
    )(parts, delta, gain, wo)[0]


def local(
    nz,
    ny,
    tokens,
    ln_gain,
    w_query_attn,
    w_key_attn,
    w_value_attn,
    w_query_delta,
    w_key_delta,
    w_value_delta,
    w_beta,
    w_decay,
    attn_bias,
    decay_log,
    beta_bias,
    log_decay_extra,
    attn_gain,
    delta_gain,
    w_out_attn,
    w_out_delta,
):
    z, y, t = lax.axis_index("z"), lax.axis_index("y"), lax.axis_index("tp")
    place = jnp.stack([z, y, t]).astype(jnp.int32)
    oa, ob = gather_weights(
        nz,
        ny,
        (w_query_attn, w_key_attn, w_value_attn),
        (w_query_delta, w_key_delta, w_value_delta, w_out_attn.T, w_out_delta.T),
    )
    oa = oa.reshape(-1, oa.shape[-1])
    ob = ob.reshape(-1, ob.shape[-1])
    qt, kv, mb, solved, qk, qd = vmem_call(
        project_kernel,
        [
            ((128, ROWS), BF16),
            ((2, ROWS, 128), BF16),
            ((128, 256), BF16),
            ((ROWS, 256), F32),
            ((ROWS, ROWS), F32),
            ((ROWS, 128), F32),
        ],
        smem=1,
        name="project",
    )(
        place,
        tokens,
        ln_gain[None],
        oa,
        ob,
        w_beta.T,
        w_decay.T,
        beta_bias[None],
        decay_log[None],
        log_decay_extra.T,
    )
    kvs, qts, mbs, totals, before = gather_keys(nz, ny, kv, qt, mb)
    bias = lax.dynamic_slice_in_dim(attn_bias, 2 * t, 2, 0)[None]
    o, sums = vmem_call(
        attend_kernel,
        [((nz, ny, 128, ROWS), BF16), ((nz, ny, 2, ROWS), F32)],
        [pltpu.VMEM((2, ROWS, ROWS), F32)] * 2 + [pltpu.VMEM((2, ROWS, ROWS), BF16)] * 2,
        smem=2,
        name="attend",
    )(place, bias, kvs, qts)
    all_sums = gather_sums(ny, sums)
    parts, delta = vmem_call(
        combine_kernel,
        [((ny, 128, ROWS), BF16), ((ROWS, 128), BF16)],
        [pltpu.VMEM((128, 128), F32), pltpu.VMEM((ny, 128, ROWS), F32)],
        smem=1,
        name="combine",
    )(place, o, all_sums, totals, before, solved, qk, qd, delta_gain[None])
    return finish(ny, lax.axis_size("tp") // 2, parts, delta, attn_gain[None], ob)


def solution(mesh):
    nz, ny = 16, 4
    split = Mesh(mesh.devices.reshape(nz, ny, mesh.shape["tp"]), ("z", "y", "tp"))
    return jax.shard_map(
        functools.partial(local, nz, ny),
        mesh=split,
        in_specs=(
            P(SP, None),
            P(),
            P(SP, "tp"),
            P(SP, "tp"),
            P(SP, "tp"),
            P(SP, "tp"),
            P(SP, "tp"),
            P(SP, "tp"),
            P(),
            P(),
            P(),
            P(),
            P(),
            P(SP, "tp"),
            P(),
            P(),
            P("tp", SP),
            P("tp", SP),
        ),
        out_specs=P(SP + ("tp",), None),
        check_vma=False,
    )
```

```python
import functools

import jax
import jax.numpy as jnp
from jax import lax
from jax.experimental import pallas as pl
from jax.experimental.pallas import tpu as pltpu
from jax.sharding import Mesh
from jax.sharding import PartitionSpec as P

MESH = pl.DeviceIdType.MESH
VMEM = pltpu.VMEM
SP = ("z", "y")
LOG2E = 1.4426950408889634
ROWS = 256
F32 = jnp.float32
BF16 = jnp.bfloat16
HIGH = lax.Precision.HIGHEST


def dot(a, b, dims=((1,), (0,)), precision=None):
    return lax.dot_general(
        a, b, (dims, ((), ())), precision=precision, preferred_element_type=F32
    )


def exact(a, b, dims=((1,), (0,))):
    return dot(a, b, dims, HIGH)


def split(a):
    high = a.astype(BF16)
    return high, (a - high.astype(F32)).astype(BF16)


def close(a, b, dims=((1,), (0,))):
    (ah, al), (bh, bl) = split(a), split(b)
    return dot(ah, bh, dims) + (dot(ah, bl, dims) + dot(al, bh, dims))


def apply_rounded(a, b):
    high, low = split(b)
    return dot(a, high) + dot(a, low)


def vmem_call(body, outs, scratch=(), smem=0, cid=None, name=None):
    params = dict(vmem_limit_bytes=60 * 1024 * 1024)
    if cid is not None:
        params.update(collective_id=cid, has_side_effects=True)

    def call(*args):
        specs = [
            pl.BlockSpec(memory_space=pltpu.SMEM if k < smem else VMEM) for k in range(len(args))
        ]
        return pl.pallas_call(
            body,
            out_shape=tuple(jax.ShapeDtypeStruct(s, d) for s, d in outs),
            in_specs=specs,
            out_specs=tuple(pl.BlockSpec(memory_space=VMEM) for _ in outs),
            scratch_shapes=list(scratch),
            compiler_params=pltpu.CompilerParams(**params),
            name=name,
        )(*args)

    return call


def places(nz, ny):
    z, y, t = lax.axis_index("z"), lax.axis_index("y"), lax.axis_index("tp")

    def at(dz, dy):
        return (lax.rem(z + (dz + nz), nz), lax.rem(y + (dy + ny), ny), t)

    return z, y, at


def remote(src, dst, ssem, rsem, device):
    return pltpu.make_async_remote_copy(
        src_ref=src, dst_ref=dst, send_sem=ssem, recv_sem=rsem, device_id=device, device_id_type=MESH
    )


def meet(peers):
    barrier = pltpu.get_barrier_semaphore()
    for peer in peers:
        pl.semaphore_signal(barrier, inc=1, device_id=peer, device_id_type=MESH)
    pl.semaphore_wait(barrier, len(peers))


class Link:
    def __init__(self, sems, own):
        self.sems, self.own, self.sent = sems, own, []

    def start(self, step, src, dst, device):
        copy = remote(src, dst, self.sems.at[0, step], self.sems.at[1, step], device)
        copy.start()
        self.sent.append(copy)

    def arrived(self, step, dst):
        remote(dst, dst, self.sems.at[0, step], self.sems.at[1, step], self.own).wait_recv()

    def drain(self):
        for copy in self.sent:
            copy.wait_send()


def weights_kernel(nz, ny, n_a, n_b, *refs):
    n = n_a + n_b
    ins, (oa, ob) = refs[:n], refs[n : n + 2]
    local, ya, za_up, za_dn, zb_up, zb_dn, y_up, y_dn, y_far = refs[n + 2 :]
    z, y, at = places(nz, ny)
    up, down, left, right = at(1, 0), at(-1, 0), at(0, -1), at(0, 1)
    row = lambda d: lax.rem(z + (d + nz), nz)
    col = lambda d: lax.rem(y + (d + ny), ny)
    ups, dns = nz // 2, nz // 2 - 1
    links = [Link(s, up) for s in (ya, za_up, za_dn, zb_up, zb_dn, y_up, y_dn, y_far)]
    ya, za_up, za_dn, zb_up, zb_dn, y_up, y_dn, y_far = links
    packs = []
    for k in range(n):
        out, place = (oa, k) if k < n_a else (ob, k - n_a)
        dst = out.at[z, y, :, pl.ds(128 * place, 128)]
        packs.append(pltpu.make_async_copy(ins[k], dst, local.at[k]))
        packs[-1].start()
    meet([up, down, left, right, at(0, 2)])
    for pack in packs:
        pack.wait()
    order = (0, 3, 1, 2)
    for d in (1, 3, 2):
        ya.start(d - 1, oa.at[z, y], oa.at[z, y], at(0, d))

    def lead(c):
        block = oa.at[z, col(c)]
        za_up.start(c, block, block, up)
        za_dn.start(c, block, block, down)

    def fan(k, zz):
        y_up.start(k, ob.at[zz, y], ob.at[zz, y], right)
        y_dn.start(k, ob.at[zz, y], ob.at[zz, y], left)

    def far(k, zz):
        y_up.arrived(k, ob.at[zz, col(-1)])
        y_dn.arrived(k, ob.at[zz, col(1)])
        if k % 2 == 0:
            y_far.start(k, ob.at[zz, col(-1)], ob.at[zz, col(-1)], right)
        else:
            y_far.start(k, ob.at[zz, col(1)], ob.at[zz, col(1)], left)

    lead(0)
    zb_up.start(0, ob.at[z, y], ob.at[z, y], up)
    zb_dn.start(0, ob.at[z, y], ob.at[z, y], down)
    fan(0, z)
    for c in order[1:]:
        ya.arrived(ny - c - 1, oa.at[z, col(c)])
        lead(c)
    waiting = [(0, z)]
    ways = ((-1, ups, zb_up, za_up, up), (1, dns, zb_dn, za_dn, down))
    for s in range(ups):
        fresh = []
        for c in order:
            for sign, steps, zb, za, to in ways:
                if s >= steps:
                    continue
                zz = row(sign * (s + 1))
                za.arrived(s * ny + c, oa.at[zz, col(c)])
                if s + 1 < steps:
                    za.start((s + 1) * ny + c, oa.at[zz, col(c)], oa.at[zz, col(c)], to)
                if c == 0:
                    zb.arrived(s, ob.at[zz, y])
                    if s + 1 < steps:
                        zb.start(s + 1, ob.at[zz, y], ob.at[zz, y], to)
                    k = 2 * s + (1 if sign < 0 else 2)
                    fan(k, zz)
                    fresh.append((k, zz))
        for k, zz in waiting:
            far(k, zz)
        waiting = fresh
    for k, zz in waiting:
        far(k, zz)
    for k in range(nz):
        y_far.arrived(k, ob.at[z, col(2)])
    for link in links:
        link.drain()


def gather_weights(nz, ny, set_a, set_b):
    sems = lambda n: pltpu.SemaphoreType.DMA((2, n))
    ups, dns = nz // 2, nz // 2 - 1
    n_a, n_b = len(set_a), len(set_b)
    rows, dtype = set_a[0].shape[0], set_a[0].dtype
    return vmem_call(
        functools.partial(weights_kernel, nz, ny, n_a, n_b),
        [((nz, ny, rows, 128 * n_a), dtype), ((nz, ny, rows, 128 * n_b), dtype)],
        [pltpu.SemaphoreType.DMA((n_a + n_b,)), sems(ny - 1), sems(ups * ny), sems(dns * ny)]
        + [sems(ups), sems(dns)]
        + [sems(nz)] * 3,
        cid=1,
        name="gather_weights",
    )(*set_a, *set_b)


def identity_part():
    rr, cc = iotas((128, 256))
    return jnp.where(rr == cc, 1.0, 0.0), cc < 128


def iotas(shape):
    return lax.broadcasted_iota(jnp.int32, shape, 0), lax.broadcasted_iota(jnp.int32, shape, 1)


def softplus(x):
    return jnp.maximum(x, 0.0) + jnp.log1p(jnp.exp(-jnp.abs(x)))


def sigmoid(x):
    return 1.0 / (1.0 + jnp.exp(-x))


def unit_rows(values):
    return values * lax.rsqrt(jnp.sum(jnp.square(values), axis=-1, keepdims=True) + 1e-06)


def project_kernel(
    tok,
    gain,
    oa,
    ob,
    w_beta,
    w_decay,
    beta_bias,
    decay_log,
    extra,
    qt,
    kv,
    mb,
    solved_ref,
    qk_ref,
    qd_ref,
):
    t = lax.axis_index("tp")
    values = tok[...].astype(F32)
    center = jnp.mean(values, axis=-1, keepdims=True)
    shifted = values - center
    spread = jnp.mean(jnp.square(shifted), axis=-1, keepdims=True)
    normed = (shifted * lax.rsqrt(spread + 1e-05) * gain[...]).astype(BF16)
    attn = dot(normed, oa[...]).astype(BF16)
    delta = dot(normed, ob[:, : 3 * 128]).astype(BF16).astype(F32)
    beta_pre = dot(normed, w_beta[...], ((1,), (1,))).astype(BF16).astype(F32)
    decay_pre = dot(normed, w_decay[...], ((1,), (1,))).astype(BF16).astype(F32)
    qt[...] = jnp.transpose(attn[:, :128].astype(F32)).astype(BF16)
    r, c = iotas((ROWS, ROWS))
    shuffle = jnp.where(c == (r & 7) * (ROWS // 8) + (r >> 3), 1.0, 0.0).astype(BF16)
    kv[0] = dot(shuffle, attn[:, 128:256]).astype(BF16)
    kv[1] = dot(shuffle, attn[:, 256:384]).astype(BF16)

    lane = lax.broadcasted_iota(jnp.int32, (1, w_beta.shape[0]), 1)

    def pick(a):
        return jnp.sum(jnp.where(lane == t, a, 0.0), axis=-1, keepdims=True)

    beta = sigmoid(pick(beta_pre) + pick(beta_bias[...]))
    rate = jnp.exp(pick(decay_log[...]))
    added = jnp.transpose(jnp.broadcast_to(extra[...], (8, ROWS)))[:, :1]
    decay = -rate * softplus(pick(decay_pre)) + added
    silu = delta * sigmoid(delta)
    queries = unit_rows(silu[:, :128]) * (128.0**-0.5)
    keys = unit_rows(silu[:, 128:256])
    vals = silu[:, 256:]
    lower = r >= c
    total = exact(jnp.where(lower, 1.0, 0.0), jnp.broadcast_to(decay, (ROWS, 128)))
    across = jnp.transpose(total)[:1, :]
    total = total[:, :1]
    end = total[ROWS - 1 :, :]
    mask = jnp.where(lower, jnp.exp(jnp.where(lower, total - across, 0.0)), 0.0)
    keys_beta = keys * beta
    grown = jnp.exp(total)
    nmat = jnp.where(r > c, close(keys_beta, keys, ((1,), (1,))) * mask, 0.0)
    near = jnp.where((r >> 3) == (c >> 3), nmat, 0.0)
    two = close(near, near)
    four = close(two, two)
    inv = jnp.where(r == c, 1.0, 0.0) - near
    inv = inv + close(inv, two)
    inv = inv + close(inv, four)
    for bit in range(3, 8):
        cross = ((r >> (bit + 1)) == (c >> (bit + 1))) & ((r >> bit) != (c >> bit))
        part = jnp.where(cross, nmat, 0.0)
        inv = inv - close(inv, close(part, inv))
    solved = close(inv, jnp.concatenate([keys_beta * grown, vals * beta], axis=1))
    solved_ref[...] = solved
    qk_ref[...] = close(queries, keys, ((1,), (1,))) * mask
    qd_ref[...] = queries * grown
    to_end = keys * jnp.exp(end - total)
    written = close(to_end, solved, ((0,), (0,)))
    eye, left_half = identity_part()
    mb[...] = jnp.where(left_half, eye * (jnp.exp(end) - 1.0) - written, written).astype(BF16)


def mixer_kernel(
    nz,
    ny,
    n_x,
    bias,
    kv,
    qt,
    mb,
    solved,
    qk,
    qd,
    delta_gain,
    attn_gain,
    wo,
    seen,
    kvs,
    qts,
    mbs,
    totals,
    before,
    kept_o,
    kept_l,
    s_even,
    s_odd,
    w_even,
    w_odd,
    state,
    acc,
    parts,
    got,
    mixed,
    mine,
    other,
    sum_ref,
    local,
    y_q,
    y_m,
    k_up,
    k_dn,
    t_up,
    t_dn,
    l_y,
    y_p,
    c_p,
    x_p,
):
    z, y, at = places(nz, ny)
    t = lax.axis_index("tp")
    x, c = lax.div(t, 2), lax.rem(t, 2)
    up, down = at(1, 0), at(-1, 0)
    row = lambda d: lax.rem(z + (d + nz), nz)
    col = lambda d: lax.rem(y + (d + ny), ny)
    far = lambda d: lax.rem(x + (d + n_x), n_x)
    in_y = lambda d: at(0, d)
    twin = (z, y, 2 * x + (1 - c))
    in_x = lambda d: (z, y, 2 * far(d) + c)
    ups, dns = nz // 2, nz // 2 - 1
    links = [Link(i, twin) for i in (y_q, y_m, t_up, t_dn, l_y, y_p, c_p, x_p)]
    y_q, y_m, t_up, t_dn, l_y, y_p, c_p, x_p = links
    k_up, k_dn = Link(k_up, twin), Link(k_dn, twin)
    meet(
        [up, down]
        + [in_y(d) for d in range(1, ny)]
        + [twin]
        + [in_x(d) for d in range(1, n_x)]
    )

    half = kv.shape[1] // 2
    part = lambda ref, p: ref.at[lax.div(p, 2), pl.ds(half * lax.rem(p, 2), half)]
    for d in (1, 3, 2):
        y_q.start(d - 1, qt, qts.at[y], in_y(d))
    for p in range(4):
        for link, to in ((k_up, up), (k_dn, down)):
            piece = kv.at[p // 2, pl.ds(half * (p % 2), half)]
            land = kvs.at[z, p // 2, pl.ds(half * (p % 2), half)]
            link.start(p, piece, land, to)
    keeps = [
        pltpu.make_async_copy(kv, kvs.at[z], local.at[0]),
        pltpu.make_async_copy(qt, qts.at[y], local.at[1]),
        pltpu.make_async_copy(mb, mbs.at[y], local.at[2]),
    ]
    for keep in keeps:
        keep.start()
    for d in (1, 3, 2):
        y_m.start(d - 1, mb, mbs.at[y], in_y(d))

    groups = ROWS // 8
    sub = lax.broadcasted_iota(jnp.int32, (8, ROWS), 0)
    query = lax.broadcasted_iota(jnp.int32, (8, ROWS), 1)

    def score(zp, yq, s):
        for h in range(2):
            s[h] = dot(kvs[zp, 0, :, h * 64 : h * 64 + 64], qts[yq, h * 64 : h * 64 + 64, :])

    def weigh(zp, yq, s, w, masked=False):
        ahead = query + ROWS * (yq - y)
        sums = []
        for h in range(2):
            run = jnp.zeros((8, ROWS), F32)
            left = [None] * groups
            for g in reversed(range(groups)):
                u = s[h, g * 8 : g * 8 + 8, :] * (0.125 * LOG2E) + bias[2 * t + h] * LOG2E
                lost = jnp.maximum(u, jnp.log2(1.0 + jnp.exp2(jnp.minimum(u, 100.0))))
                if masked:
                    lost = jnp.where(sub * groups + g < ahead, lost, 0.0)
                run = run + lost
                left[g] = u - run
            incl = run
            for d in (1, 2, 4):
                incl = incl + jnp.where(sub < 8 - d, pltpu.roll(incl, 8 - d, 0), 0.0)
            later = jnp.where(sub < 7, pltpu.roll(incl, 7, 0), 0.0)
            for g in range(0, groups, 2):
                pair = [jnp.exp2(left[j] - later) for j in (g, g + 1)]
                if masked:
                    pair = [
                        jnp.where(sub * groups + j < ahead, e, 0.0) for e, j in zip(pair, (g, g + 1))
                    ]
                w[h, g * 8 : g * 8 + 16, :] = jnp.concatenate(pair, axis=0).astype(BF16)
            sums.append(incl[:1])
        kept_l[y, zp, yq] = jnp.concatenate(sums, axis=0)

    def apply(zp, yq, w):
        for h in range(2):
            kept_o[zp, yq, h * 64 : h * 64 + 64, :] = dot(
                kvs[zp, 1, :, h * 64 : h * 64 + 64], w[h], ((0,), (0,))
            )

    def send_sums(block, zz):
        for d in (1, 3, 2):
            l_y.start(3 * block + d - 1, kept_l.at[y, zz], kept_l.at[y, zz], in_y(d))

    def forward(s, p):
        for sign, steps, link, to in ((-1, ups, k_up, up), (1, dns, k_dn, down)):
            if s < steps:
                block = part(kvs.at[row(sign * (s + 1))], p)
                link.arrived(4 * s + p, block)
                if s + 1 < steps:
                    step = 4 * (s + 1) + p
                    remote(block, block, link.sems.at[0, step], link.sems.at[1, step], to).start()

    t_rows = totals.shape[1] // 2
    piece = lambda zz, p: totals.at[zz, pl.ds(t_rows * p, t_rows)]

    def forward_totals(j):
        for sign, steps, link, to in ((-1, ups, t_up, up), (1, dns, t_dn, down)):
            if j < steps:
                zz = row(sign * (j + 1))
                for p in range(2):
                    link.arrived(2 * j + p, piece(zz, p))
                    if j + 1 < steps:
                        link.start(2 * (j + 1) + p, piece(zz, p), piece(zz, p), to)

    @pl.loop(0, 4)
    def _(p):
        forward(0, p)

    for d in (1, 3, 2):
        y_q.arrived(d - 1, qts.at[col(-d)])
    keeps[0].wait()
    keeps[1].wait()
    w_odd[...] = jnp.zeros_like(w_odd)
    score(z, 0, s_even)

    @pl.loop(0, ny // 2)
    def _(m):
        yq = 2 * m
        score(z, yq + 1, s_odd)
        weigh(z, yq, s_even, w_even, True)
        apply(z, jnp.maximum(yq - 1, 0), w_odd)
        score(z, jnp.minimum(yq + 2, ny - 1), s_even)
        weigh(z, yq + 1, s_odd, w_odd, True)
        apply(z, yq, w_even)

    apply(z, ny - 1, w_odd)
    score(row(-1), 0, s_even)

    for s in range(1, ups):
        if s == 1:
            for d in (1, 3, 2):
                y_m.arrived(d - 1, mbs.at[col(-d)])
            keeps[2].wait()
            eye, left_half = identity_part()
            chain, first = eye, eye
            for k in range(ny):
                m = mbs[k]
                first = jnp.where(y == k, chain, first)
                shift = chain + jnp.where(left_half, 0.0, m.astype(F32))
                chain = apply_rounded(m[:, :128], chain) + shift
            before[...] = first
            totals[z] = (chain - eye).astype(BF16)
        one, two = row(-s), row(s)
        last = two if s == 1 else row(s - 1)
        ahead = row(-s - 1)

        @pl.loop(0, ny)
        def _(p):
            forward(s, p)
            at_start, at_end = p == 0, p == ny - 1
            score(two, p, s_odd)
            weigh(one, p, s_even, w_even)
            apply(jnp.where(at_start, last, two), lax.rem(p + ny - 1, ny), w_odd)
            score(jnp.where(at_end, ahead, one), lax.rem(p + 1, ny), s_even)
            weigh(two, p, s_odd, w_odd)
            apply(one, p, w_even)

        if s == 1:
            for p in range(2):
                t_up.start(p, piece(z, p), piece(z, p), up)
                t_dn.start(p, piece(z, p), piece(z, p), down)
            send_sums(0, z)
        else:
            forward_totals(s - 2)
            send_sums(2 * s - 3, row(1 - s))
            send_sums(2 * s - 2, row(s - 1))

    one, two = row(-ups), row(ups - 1)
    score(one, 1, s_odd)
    weigh(one, 0, s_even, w_even)
    apply(two, ny - 1, w_odd)
    send_sums(2 * ups - 3, row(1 - ups))
    send_sums(2 * ups - 2, row(ups - 1))
    forward_totals(ups - 2)
    score(one, 2, s_even)
    weigh(one, 1, s_odd, w_odd)
    apply(one, 0, w_even)
    score(one, 3, s_odd)
    weigh(one, 2, s_even, w_even)
    apply(one, 1, w_odd)
    weigh(one, 3, s_odd, w_odd)
    apply(one, 2, w_even)
    apply(one, 3, w_odd)
    forward_totals(ups - 1)
    send_sums(2 * ups - 1, one)

    state[...] = jnp.zeros_like(state)

    @pl.loop(0, z)
    def _(k):
        now = state[...]
        state[...] = now + apply_rounded(totals[k, :, :128], now) + totals[k, :, 128:].astype(F32)

    incoming = close(before[:, :128], state[...]) + before[:, 128:]
    fresh = solved[:, 128:] - close(solved[:, :128], incoming)
    raw = close(qd[...], incoming) + close(qk[...], fresh)
    scale = lax.rsqrt(jnp.mean(jnp.square(raw), axis=-1, keepdims=True) + 1e-06)
    rows = seen.shape[1]
    delta = (raw * scale * delta_gain[...]).astype(BF16)
    mixed[:, :, :, 128:] = delta.reshape(n_x, 2, rows, 128)

    blocks = [(0, z)] + [(1 + 2 * j, row(-1 - j)) for j in range(ups)]
    blocks += [(2 + 2 * j, row(1 + j)) for j in range(dns)]
    for block, zz in blocks:
        for d in (1, 3, 2):
            l_y.arrived(3 * block + d - 1, kept_l.at[col(-d), zz])
    acc[...] = jnp.zeros_like(acc)

    def rescale(i, later):
        zp = z - i
        sums = [kept_l[k, zp] for k in range(ny)]
        here = later
        for k in range(ny):
            here = here + jnp.where(k > y, sums[k], 0.0)
            later = later + sums[k]
        kept = jnp.exp2(-here)
        for yq in range(ny):
            for h in range(2):
                part_rows = slice(h * 64, h * 64 + 64)
                acc[yq, part_rows, :] += kept_o[zp, yq, part_rows, :] * kept[yq, h : h + 1, :]
        return later

    lax.fori_loop(0, z + 1, rescale, jnp.zeros(kept_l.shape[2:], F32))
    parts[...] = acc[...].astype(BF16)
    raw = acc[y]
    for d in (1, 3, 2):
        y_p.start(d - 1, parts.at[col(d)], got.at[y], in_y(d))
    for d in (1, 3, 2):
        y_p.arrived(d - 1, got.at[col(-d)])
        raw = raw + got[col(-d)].astype(F32)
    halves = []
    for h in range(2):
        piece_h = raw[h * 64 : h * 64 + 64]
        power = jnp.mean(jnp.square(piece_h), axis=0, keepdims=True)
        halves.append(piece_h * lax.rsqrt(power + 1e-06))
    gains = jnp.concatenate([attn_gain[...], attn_gain[...]], axis=1)
    attn = (jnp.transpose(jnp.concatenate(halves, axis=0)) * gains).astype(BF16)
    mixed[:, :, :, :128] = attn.reshape(n_x, 2, rows, 128)

    def product(core):
        picked = mixed[:, core].reshape(n_x * rows, 256)
        return dot(picked, wo[:, 3 * 128 :], ((1,), (1,))).astype(BF16).reshape(n_x, rows, -1)

    mine[...] = product(1 - c)
    own = product(c)
    c_p.start(0, mine, other, twin)
    sum_ref[...] = own
    c_p.arrived(0, other)
    for d in (2, 1, 3):
        sum_ref[far(d)] = (sum_ref[far(d)].astype(F32) + other[far(d)].astype(F32)).astype(BF16)
    seen[x] = (sum_ref[x].astype(F32) + other[x].astype(F32)).astype(BF16)
    for d in (2, 1, 3):
        x_p.start(d - 1, sum_ref.at[far(d)], seen.at[x], in_x(d))
    for d in (1, 3, 2):
        x_p.arrived(d - 1, seen.at[far(-d)])
    for link in links:
        link.drain()
    for link, steps in ((k_up, ups), (k_dn, dns)):

        @pl.loop(0, 4 * steps)
        def _(k):
            block = part(kvs.at[z], lax.rem(k, 4))
            remote(block, block, link.sems.at[0, k], link.sems.at[1, k], twin).wait_send()


def mix(nz, ny, n_x, bias, kv, qt, mb, solved, qk, qd, delta_gain, attn_gain, wo):
    rows, wide = ROWS // (2 * n_x), wo.shape[0]
    sems = lambda n: pltpu.SemaphoreType.DMA((2, n))
    big = pltpu.VMEM((n_x, rows, wide), BF16)
    ups, dns = nz // 2, nz // 2 - 1
    return vmem_call(
        functools.partial(mixer_kernel, nz, ny, n_x),
        [((n_x, rows, wide), BF16)],
        [
            pltpu.VMEM((nz,) + kv.shape, BF16),
            pltpu.VMEM((ny,) + qt.shape, BF16),
            pltpu.VMEM((ny,) + mb.shape, BF16),
            pltpu.VMEM((nz,) + mb.shape, BF16),
            pltpu.VMEM(mb.shape, F32),
            pltpu.VMEM((nz, ny, 128, ROWS), F32),
            pltpu.VMEM((ny, nz, ny, 2, ROWS), F32),
            pltpu.VMEM((2, ROWS, ROWS), F32),
            pltpu.VMEM((2, ROWS, ROWS), F32),
            pltpu.VMEM((2, ROWS, ROWS), BF16),
            pltpu.VMEM((2, ROWS, ROWS), BF16),
            pltpu.VMEM((128, 128), F32),
            pltpu.VMEM((ny, 128, ROWS), F32),
            pltpu.VMEM((ny, 128, ROWS), BF16),
            pltpu.VMEM((ny, 128, ROWS), BF16),
            pltpu.VMEM((n_x, 2, rows, 256), BF16),
            big,
            big,
            big,
            pltpu.SemaphoreType.DMA((3,)),
            sems(ny - 1),
            sems(ny - 1),
            sems(4 * ups),
            sems(4 * dns),
            sems(2 * ups),
            sems(2 * dns),
            sems((ny - 1) * nz),
            sems(ny - 1),
            sems(1),
            sems(n_x - 1),
        ],
        smem=1,
        cid=2,
        name="mixer",
    )(bias, kv, qt, mb, solved, qk, qd, delta_gain, attn_gain, wo)[0]


def local(
    nz,
    ny,
    tokens,
    ln_gain,
    w_query_attn,
    w_key_attn,
    w_value_attn,
    w_query_delta,
    w_key_delta,
    w_value_delta,
    w_beta,
    w_decay,
    attn_bias,
    decay_log,
    beta_bias,
    log_decay_extra,
    attn_gain,
    delta_gain,
    w_out_attn,
    w_out_delta,
):
    oa, ob = gather_weights(
        nz,
        ny,
        (w_query_attn, w_key_attn, w_value_attn),
        (w_query_delta, w_key_delta, w_value_delta, w_out_attn.T, w_out_delta.T),
    )
    oa = oa.reshape(-1, oa.shape[-1])
    ob = ob.reshape(-1, ob.shape[-1])
    qt, kv, mb, solved, qk, qd = vmem_call(
        project_kernel,
        [
            ((128, ROWS), BF16),
            ((2, ROWS, 128), BF16),
            ((128, 256), BF16),
            ((ROWS, 256), F32),
            ((ROWS, ROWS), F32),
            ((ROWS, 128), F32),
        ],
        name="project",
    )(
        tokens,
        ln_gain[None],
        oa,
        ob,
        w_beta.T,
        w_decay.T,
        beta_bias[None],
        decay_log[None],
        log_decay_extra.T,
    )
    pieces = mix(
        nz,
        ny,
        lax.axis_size("tp") // 2,
        attn_bias,
        kv,
        qt,
        mb,
        solved,
        qk,
        qd,
        delta_gain[None],
        attn_gain[None],
        ob,
    )
    return jnp.sum(pieces.astype(F32), axis=0).astype(BF16)


def solution(mesh):
    nz, ny = 16, 4
    split = Mesh(mesh.devices.reshape(nz, ny, mesh.shape["tp"]), ("z", "y", "tp"))
    return jax.shard_map(
        functools.partial(local, nz, ny),
        mesh=split,
        in_specs=(
            P(SP, None),
            P(),
            P(SP, "tp"),
            P(SP, "tp"),
            P(SP, "tp"),
            P(SP, "tp"),
            P(SP, "tp"),
            P(SP, "tp"),
            P(),
            P(),
            P(),
            P(),
            P(),
            P(SP, "tp"),
            P(),
            P(),
            P("tp", SP),
            P("tp", SP),
        ),
        out_specs=P(SP + ("tp",), None),
        check_vma=False,
    )
```

```python
import functools

import jax
import jax.numpy as jnp
from jax import lax
from jax.experimental import pallas as pl
from jax.experimental.pallas import tpu as pltpu
from jax.sharding import Mesh
from jax.sharding import PartitionSpec as P

MESH = pl.DeviceIdType.MESH
VMEM = pltpu.VMEM
SP = ("z", "y")
LOG2E = 1.4426950408889634
ROWS = 256
F32 = jnp.float32
BF16 = jnp.bfloat16
HIGH = lax.Precision.HIGHEST


def dot(a, b, dims=((1,), (0,)), precision=None):
    return lax.dot_general(
        a, b, (dims, ((), ())), precision=precision, preferred_element_type=F32
    )


def exact(a, b, dims=((1,), (0,))):
    return dot(a, b, dims, HIGH)


def split(a):
    high = a.astype(BF16)
    return high, (a - high.astype(F32)).astype(BF16)


def close(a, b, dims=((1,), (0,))):
    (ah, al), (bh, bl) = split(a), split(b)
    return dot(ah, bh, dims) + (dot(ah, bl, dims) + dot(al, bh, dims))


def apply_rounded(a, b):
    high, low = split(b)
    return dot(a, high) + dot(a, low)


def vmem_call(body, outs, scratch=(), smem=0, cid=None, name=None):
    params = dict(vmem_limit_bytes=60 * 1024 * 1024)
    if cid is not None:
        params.update(collective_id=cid, has_side_effects=True)

    def call(*args):
        specs = [
            pl.BlockSpec(memory_space=pltpu.SMEM if k < smem else VMEM) for k in range(len(args))
        ]
        return pl.pallas_call(
            body,
            out_shape=tuple(jax.ShapeDtypeStruct(s, d) for s, d in outs),
            in_specs=specs,
            out_specs=tuple(pl.BlockSpec(memory_space=VMEM) for _ in outs),
            scratch_shapes=list(scratch),
            compiler_params=pltpu.CompilerParams(**params),
            name=name,
        )(*args)

    return call


def places(nz, ny):
    z, y, t = lax.axis_index("z"), lax.axis_index("y"), lax.axis_index("tp")

    def at(dz, dy):
        return (lax.rem(z + (dz + nz), nz), lax.rem(y + (dy + ny), ny), t)

    return z, y, at


def remote(src, dst, ssem, rsem, device):
    return pltpu.make_async_remote_copy(
        src_ref=src, dst_ref=dst, send_sem=ssem, recv_sem=rsem, device_id=device, device_id_type=MESH
    )


def meet(peers):
    barrier = pltpu.get_barrier_semaphore()
    for peer in peers:
        pl.semaphore_signal(barrier, inc=1, device_id=peer, device_id_type=MESH)
    pl.semaphore_wait(barrier, len(peers))


class Link:
    def __init__(self, sems, own):
        self.sems, self.own, self.sent = sems, own, []

    def start(self, step, src, dst, device):
        copy = remote(src, dst, self.sems.at[0, step], self.sems.at[1, step], device)
        copy.start()
        self.sent.append(copy)

    def arrived(self, step, dst):
        remote(dst, dst, self.sems.at[0, step], self.sems.at[1, step], self.own).wait_recv()

    def drain(self):
        for copy in self.sent:
            copy.wait_send()


def identity_part():
    rr, cc = iotas((128, 256))
    return jnp.where(rr == cc, 1.0, 0.0), cc < 128


def iotas(shape):
    return lax.broadcasted_iota(jnp.int32, shape, 0), lax.broadcasted_iota(jnp.int32, shape, 1)


def softplus(x):
    return jnp.maximum(x, 0.0) + jnp.log1p(jnp.exp(-jnp.abs(x)))


def sigmoid(x):
    return 1.0 / (1.0 + jnp.exp(-x))


def unit_rows(values):
    return values * lax.rsqrt(jnp.sum(jnp.square(values), axis=-1, keepdims=True) + 1e-06)


SCRATCH = (
    "oa",
    "ob",
    "normed",
    "kvs",
    "qts",
    "mbs",
    "totals",
    "before",
    "solved",
    "qk_part",
    "qd",
    "kept_o",
    "kept_l",
    "s_even",
    "s_odd",
    "w_even",
    "w_odd",
    "state",
    "acc",
    "parts",
    "got",
    "mixed",
    "mine",
    "other",
    "sum_ref",
    "local",
    "ya",
    "za_up",
    "za_dn",
    "zb_up",
    "zb_dn",
    "y_up",
    "y_dn",
    "y_far",
    "y_q",
    "y_m",
    "k_up",
    "k_dn",
    "t_up",
    "t_dn",
    "l_y",
    "y_p",
    "c_p",
    "x_p",
)


def layer_kernel(nz, ny, n_x, n_a, n_b, attn_bias, tok, ln_gain, *refs):
    n = n_a + n_b
    ins, refs = refs[:n], refs[n:]
    w_beta, w_decay, beta_bias, decay_log, extra, delta_gain, attn_gain, seen = refs[:8]
    r_ = dict(zip(SCRATCH, refs[8:]))
    oa, ob, normed_ref, kvs, qts, mbs, totals, before, solved, qk, qd = [
        r_[k] for k in SCRATCH[:11]
    ]
    kept_o, kept_l, s_even, s_odd, w_even, w_odd = [r_[k] for k in SCRATCH[11:17]]
    state, acc, parts, got, mixed, mine, other, sum_ref, local = [r_[k] for k in SCRATCH[17:26]]
    z, y, at = places(nz, ny)
    t = lax.axis_index("tp")
    x, c = lax.div(t, 2), lax.rem(t, 2)
    up, down, left, right = at(1, 0), at(-1, 0), at(0, -1), at(0, 1)
    row = lambda d: lax.rem(z + (d + nz), nz)
    col = lambda d: lax.rem(y + (d + ny), ny)
    far = lambda d: lax.rem(x + (d + n_x), n_x)
    in_y = lambda d: at(0, d)
    twin = (z, y, 2 * x + (1 - c))
    in_x = lambda d: (z, y, 2 * far(d) + c)
    ups, dns = nz // 2, nz // 2 - 1
    every = {k: Link(r_[k], twin) for k in SCRATCH[26:]}
    links = [every[k] for k in SCRATCH[26:] if k not in ("k_up", "k_dn")]
    ya, za_up, za_dn, zb_up, zb_dn, y_up, y_dn, y_far = [every[k] for k in SCRATCH[26:34]]
    y_q, y_m, k_up, k_dn, t_up, t_dn, l_y, y_p, c_p, x_p = [every[k] for k in SCRATCH[34:]]
    packs = []
    for k in range(n):
        out, place = (oa, k) if k < n_a else (ob, k - n_a)
        dst = out.at[z, y, :, pl.ds(128 * place, 128)]
        packs.append(pltpu.make_async_copy(ins[k], dst, local.at[k]))
        packs[-1].start()
    meet(
        [up, down]
        + [in_y(d) for d in range(1, ny)]
        + [twin]
        + [in_x(d) for d in range(1, n_x)]
    )
    for pack in packs:
        pack.wait()
    order = (0, 3, 1, 2)
    for d in (1, 3, 2):
        ya.start(d - 1, oa.at[z, y], oa.at[z, y], at(0, d))

    def lead(c):
        block = oa.at[z, col(c)]
        za_up.start(c, block, block, up)
        za_dn.start(c, block, block, down)

    def fan(k, zz):
        y_up.start(k, ob.at[zz, y], ob.at[zz, y], right)
        y_dn.start(k, ob.at[zz, y], ob.at[zz, y], left)

    def relay(k, zz):
        y_up.arrived(k, ob.at[zz, col(-1)])
        y_dn.arrived(k, ob.at[zz, col(1)])
        if k % 2 == 0:
            y_far.start(k, ob.at[zz, col(-1)], ob.at[zz, col(-1)], right)
        else:
            y_far.start(k, ob.at[zz, col(1)], ob.at[zz, col(1)], left)

    lead(0)
    zb_up.start(0, ob.at[z, y], ob.at[z, y], up)
    zb_dn.start(0, ob.at[z, y], ob.at[z, y], down)
    fan(0, z)
    values = tok[...].astype(F32)
    center = jnp.mean(values, axis=-1, keepdims=True)
    shifted = values - center
    spread = jnp.mean(jnp.square(shifted), axis=-1, keepdims=True)
    normed_ref[...] = (shifted * lax.rsqrt(spread + 1e-05) * ln_gain[...]).astype(BF16)
    for c_ in order[1:]:
        ya.arrived(ny - c_ - 1, oa.at[z, col(c_)])
        lead(c_)
    waiting = [(0, z)]
    ways = ((-1, ups, zb_up, za_up, up), (1, dns, zb_dn, za_dn, down))
    for s in range(ups):
        fresh = []
        for c_ in order:
            for sign, steps, zb, za, to in ways:
                if s >= steps:
                    continue
                zz = row(sign * (s + 1))
                za.arrived(s * ny + c_, oa.at[zz, col(c_)])
                if s + 1 < steps:
                    za.start((s + 1) * ny + c_, oa.at[zz, col(c_)], oa.at[zz, col(c_)], to)
                if c_ == 0:
                    zb.arrived(s, ob.at[zz, y])
                    if s + 1 < steps:
                        zb.start(s + 1, ob.at[zz, y], ob.at[zz, y], to)
                    k = 2 * s + (1 if sign < 0 else 2)
                    fan(k, zz)
                    fresh.append((k, zz))
        for k, zz in waiting:
            relay(k, zz)
        waiting = fresh
    for k, zz in waiting:
        relay(k, zz)

    normed = normed_ref[...]
    weights_a = oa[...].reshape(-1, 128 * n_a)
    attn = dot(normed, weights_a).astype(BF16)
    qts[y] = jnp.transpose(attn[:, :128].astype(F32)).astype(BF16)
    r, c_ = iotas((ROWS, ROWS))
    shuffle = jnp.where(c_ == (r & 7) * (ROWS // 8) + (r >> 3), 1.0, 0.0).astype(BF16)
    kvs[z, 0] = dot(shuffle, attn[:, 128:256]).astype(BF16)
    kvs[z, 1] = dot(shuffle, attn[:, 256:384]).astype(BF16)
    beta_pre = dot(normed, w_beta[...], ((1,), (1,))).astype(BF16).astype(F32)
    decay_pre = dot(normed, w_decay[...], ((1,), (1,))).astype(BF16).astype(F32)
    for k in range(nz):
        y_far.arrived(k, ob.at[z, col(2)])
    half = ROWS // 2
    part = lambda ref, p: ref.at[lax.div(p, 2), pl.ds(half * lax.rem(p, 2), half)]
    for d in (1, 3, 2):
        y_q.start(d - 1, qts.at[y], qts.at[y], in_y(d))
    for p in range(4):
        for link, to in ((k_up, up), (k_dn, down)):
            block = kvs.at[z, p // 2, pl.ds(half * (p % 2), half)]
            remote(block, block, link.sems.at[0, p], link.sems.at[1, p], to).start()
    delta = dot(normed, ob[:, :, :, : 3 * 128].reshape(-1, 384)).astype(BF16).astype(F32)

    groups = ROWS // 8
    sub = lax.broadcasted_iota(jnp.int32, (8, ROWS), 0)
    query = lax.broadcasted_iota(jnp.int32, (8, ROWS), 1)

    def score(zp, yq, s):
        for h in range(2):
            s[h] = dot(kvs[zp, 0, :, h * 64 : h * 64 + 64], qts[yq, h * 64 : h * 64 + 64, :])

    def weigh(zp, yq, s, w, masked=False):
        ahead = query + ROWS * (yq - y)
        sums = []
        for h in range(2):
            run = jnp.zeros((8, ROWS), F32)
            left = [None] * groups
            for g in reversed(range(groups)):
                u = s[h, g * 8 : g * 8 + 8, :] * (0.125 * LOG2E) + attn_bias[2 * t + h] * LOG2E
                lost = jnp.maximum(u, jnp.log2(1.0 + jnp.exp2(jnp.minimum(u, 100.0))))
                if masked:
                    lost = jnp.where(sub * groups + g < ahead, lost, 0.0)
                run = run + lost
                left[g] = u - run
            incl = run
            for d in (1, 2, 4):
                incl = incl + jnp.where(sub < 8 - d, pltpu.roll(incl, 8 - d, 0), 0.0)
            later = jnp.where(sub < 7, pltpu.roll(incl, 7, 0), 0.0)
            for g in range(0, groups, 2):
                pair = [jnp.exp2(left[j] - later) for j in (g, g + 1)]
                if masked:
                    pair = [
                        jnp.where(sub * groups + j < ahead, e, 0.0) for e, j in zip(pair, (g, g + 1))
                    ]
                w[h, g * 8 : g * 8 + 16, :] = jnp.concatenate(pair, axis=0).astype(BF16)
            sums.append(incl[:1])
        kept_l[y, zp, yq] = jnp.concatenate(sums, axis=0)

    def apply(zp, yq, w):
        for h in range(2):
            kept_o[zp, yq, h * 64 : h * 64 + 64, :] = dot(
                kvs[zp, 1, :, h * 64 : h * 64 + 64], w[h], ((0,), (0,))
            )

    def send_sums(block, zz):
        for d in (1, 3, 2):
            l_y.start(3 * block + d - 1, kept_l.at[y, zz], kept_l.at[y, zz], in_y(d))

    def forward(s, p):
        for sign, steps, link, to in ((-1, ups, k_up, up), (1, dns, k_dn, down)):
            if s < steps:
                block = part(kvs.at[row(sign * (s + 1))], p)
                link.arrived(4 * s + p, block)
                if s + 1 < steps:
                    step = 4 * (s + 1) + p
                    remote(block, block, link.sems.at[0, step], link.sems.at[1, step], to).start()

    t_rows = totals.shape[1] // 2
    piece = lambda zz, p: totals.at[zz, pl.ds(t_rows * p, t_rows)]

    def forward_totals(j):
        for sign, steps, link, to in ((-1, ups, t_up, up), (1, dns, t_dn, down)):
            if j < steps:
                zz = row(sign * (j + 1))
                for p in range(2):
                    link.arrived(2 * j + p, piece(zz, p))
                    if j + 1 < steps:
                        link.start(2 * (j + 1) + p, piece(zz, p), piece(zz, p), to)

    lane = lax.broadcasted_iota(jnp.int32, (1, w_beta.shape[0]), 1)

    def pick(a):
        return jnp.sum(jnp.where(lane == t, a, 0.0), axis=-1, keepdims=True)

    beta = sigmoid(pick(beta_pre) + pick(beta_bias[...]))
    rate = jnp.exp(pick(decay_log[...]))
    added = jnp.transpose(jnp.broadcast_to(extra[...], (8, ROWS)))[:, :1]
    decay = -rate * softplus(pick(decay_pre)) + added
    silu = delta * sigmoid(delta)
    queries = unit_rows(silu[:, :128]) * (128.0**-0.5)
    keys = unit_rows(silu[:, 128:256])
    vals = silu[:, 256:]
    lower = r >= c_
    total = exact(jnp.where(lower, 1.0, 0.0), jnp.broadcast_to(decay, (ROWS, 128)))
    across = jnp.transpose(total)[:1, :]
    total = total[:, :1]
    end = total[ROWS - 1 :, :]
    mask = jnp.where(lower, jnp.exp(jnp.where(lower, total - across, 0.0)), 0.0)
    keys_beta = keys * beta
    grown = jnp.exp(total)
    nmat = jnp.where(r > c_, close(keys_beta, keys, ((1,), (1,))) * mask, 0.0)
    near = jnp.where((r >> 3) == (c_ >> 3), nmat, 0.0)
    two = close(near, near)
    four = close(two, two)
    inv = jnp.where(r == c_, 1.0, 0.0) - near
    inv = inv + close(inv, two)
    inv = inv + close(inv, four)

    @pl.loop(0, 4)
    def _(p):
        forward(0, p)

    for bit in range(3, 8):
        cross = ((r >> (bit + 1)) == (c_ >> (bit + 1))) & ((r >> bit) != (c_ >> bit))
        band = jnp.where(cross, nmat, 0.0)
        inv = inv - close(inv, close(band, inv))
    answer = close(inv, jnp.concatenate([keys_beta * grown, vals * beta], axis=1))
    solved[...] = answer
    to_end = keys * jnp.exp(end - total)
    written = close(to_end, answer, ((0,), (0,)))
    eye, left_half = identity_part()
    mbs[y] = jnp.where(left_half, eye * (jnp.exp(end) - 1.0) - written, written).astype(BF16)
    qk[...] = close(queries, keys, ((1,), (1,))) * mask
    qd[...] = queries * grown
    for d in (1, 3, 2):
        y_m.start(d - 1, mbs.at[y], mbs.at[y], in_y(d))

    for d in (1, 3, 2):
        y_q.arrived(d - 1, qts.at[col(-d)])
    w_odd[...] = jnp.zeros_like(w_odd)
    score(z, 0, s_even)

    @pl.loop(0, ny // 2)
    def _(m):
        yq = 2 * m
        score(z, yq + 1, s_odd)
        weigh(z, yq, s_even, w_even, True)
        apply(z, jnp.maximum(yq - 1, 0), w_odd)
        score(z, jnp.minimum(yq + 2, ny - 1), s_even)
        weigh(z, yq + 1, s_odd, w_odd, True)
        apply(z, yq, w_even)

    apply(z, ny - 1, w_odd)
    score(row(-1), 0, s_even)

    for s in range(1, ups):
        if s == 1:
            for d in (1, 3, 2):
                y_m.arrived(d - 1, mbs.at[col(-d)])
            eye, left_half = identity_part()
            chain, first = eye, eye
            for k in range(ny):
                m = mbs[k]
                first = jnp.where(y == k, chain, first)
                shift = chain + jnp.where(left_half, 0.0, m.astype(F32))
                chain = apply_rounded(m[:, :128], chain) + shift
            before[...] = first
            totals[z] = (chain - eye).astype(BF16)
        one, two = row(-s), row(s)
        last = two if s == 1 else row(s - 1)
        ahead = row(-s - 1)

        @pl.loop(0, ny)
        def _(p):
            forward(s, p)
            at_start, at_end = p == 0, p == ny - 1
            score(two, p, s_odd)
            weigh(one, p, s_even, w_even)
            apply(jnp.where(at_start, last, two), lax.rem(p + ny - 1, ny), w_odd)
            score(jnp.where(at_end, ahead, one), lax.rem(p + 1, ny), s_even)
            weigh(two, p, s_odd, w_odd)
            apply(one, p, w_even)

        if s == 1:
            for p in range(2):
                t_up.start(p, piece(z, p), piece(z, p), up)
                t_dn.start(p, piece(z, p), piece(z, p), down)
            send_sums(0, z)
        else:
            forward_totals(s - 2)
            send_sums(2 * s - 3, row(1 - s))
            send_sums(2 * s - 2, row(s - 1))

    one, two = row(-ups), row(ups - 1)
    score(one, 1, s_odd)
    weigh(one, 0, s_even, w_even)
    apply(two, ny - 1, w_odd)
    send_sums(2 * ups - 3, row(1 - ups))
    send_sums(2 * ups - 2, row(ups - 1))
    forward_totals(ups - 2)
    score(one, 2, s_even)
    weigh(one, 1, s_odd, w_odd)
    apply(one, 0, w_even)
    score(one, 3, s_odd)
    weigh(one, 2, s_even, w_even)
    apply(one, 1, w_odd)
    weigh(one, 3, s_odd, w_odd)
    apply(one, 2, w_even)
    apply(one, 3, w_odd)
    forward_totals(ups - 1)
    send_sums(2 * ups - 1, one)

    state[...] = jnp.zeros_like(state)

    @pl.loop(0, z)
    def _(k):
        now = state[...]
        state[...] = now + apply_rounded(totals[k, :, :128], now) + totals[k, :, 128:].astype(F32)

    incoming = close(before[:, :128], state[...]) + before[:, 128:]
    fresh = solved[:, 128:] - close(solved[:, :128], incoming)
    raw = close(qd[...], incoming) + close(qk[...], fresh)
    scale = lax.rsqrt(jnp.mean(jnp.square(raw), axis=-1, keepdims=True) + 1e-06)
    rows = seen.shape[1]
    delta = (raw * scale * delta_gain[...]).astype(BF16)
    mixed[:, :, :, 128:] = delta.reshape(n_x, 2, rows, 128)

    blocks = [(0, z)] + [(1 + 2 * j, row(-1 - j)) for j in range(ups)]
    blocks += [(2 + 2 * j, row(1 + j)) for j in range(dns)]
    for block, zz in blocks:
        for d in (1, 3, 2):
            l_y.arrived(3 * block + d - 1, kept_l.at[col(-d), zz])
    acc[...] = jnp.zeros_like(acc)

    def rescale(i, later):
        zp = z - i
        sums = [kept_l[k, zp] for k in range(ny)]
        here = later
        for k in range(ny):
            here = here + jnp.where(k > y, sums[k], 0.0)
            later = later + sums[k]
        kept = jnp.exp2(-here)
        for yq in range(ny):
            for h in range(2):
                part_rows = slice(h * 64, h * 64 + 64)
                acc[yq, part_rows, :] += kept_o[zp, yq, part_rows, :] * kept[yq, h : h + 1, :]
        return later

    lax.fori_loop(0, z + 1, rescale, jnp.zeros(kept_l.shape[2:], F32))
    parts[...] = acc[...].astype(BF16)
    raw = acc[y]
    for d in (1, 3, 2):
        y_p.start(d - 1, parts.at[col(d)], got.at[y], in_y(d))
    for d in (1, 3, 2):
        y_p.arrived(d - 1, got.at[col(-d)])
        raw = raw + got[col(-d)].astype(F32)
    halves = []
    for h in range(2):
        piece_h = raw[h * 64 : h * 64 + 64]
        power = jnp.mean(jnp.square(piece_h), axis=0, keepdims=True)
        halves.append(piece_h * lax.rsqrt(power + 1e-06))
    gains = jnp.concatenate([attn_gain[...], attn_gain[...]], axis=1)
    attn = (jnp.transpose(jnp.concatenate(halves, axis=0)) * gains).astype(BF16)
    mixed[:, :, :, :128] = attn.reshape(n_x, 2, rows, 128)

    def product(core):
        picked = mixed[:, core].reshape(n_x * rows, 256)
        return dot(picked, ob[:, :, :, 3 * 128 :].reshape(-1, 256), ((1,), (1,))).astype(BF16).reshape(n_x, rows, -1)

    mine[...] = product(1 - c)
    own = product(c)
    c_p.start(0, mine, other, twin)
    sum_ref[...] = own
    c_p.arrived(0, other)
    for d in (2, 1, 3):
        sum_ref[far(d)] = (sum_ref[far(d)].astype(F32) + other[far(d)].astype(F32)).astype(BF16)
    seen[x] = (sum_ref[x].astype(F32) + other[x].astype(F32)).astype(BF16)
    for d in (2, 1, 3):
        x_p.start(d - 1, sum_ref.at[far(d)], seen.at[x], in_x(d))
    for d in (1, 3, 2):
        x_p.arrived(d - 1, seen.at[far(-d)])
    for link in links:
        link.drain()
    for link, steps in ((k_up, ups), (k_dn, dns)):

        @pl.loop(0, 4 * steps)
        def _(k):
            block = part(kvs.at[z], lax.rem(k, 4))
            remote(block, block, link.sems.at[0, k], link.sems.at[1, k], twin).wait_send()


def layer(nz, ny, n_x, attn_bias, tok, ln_gain, set_a, set_b, *rest):
    n_a, n_b = len(set_a), len(set_b)
    w_rows, wide = set_a[0].shape[0], nz * ny * set_a[0].shape[0]
    rows = ROWS // (2 * n_x)
    sems = lambda n: pltpu.SemaphoreType.DMA((2, n))
    f32 = lambda *shape: pltpu.VMEM(shape, F32)
    b16 = lambda *shape: pltpu.VMEM(shape, BF16)
    ups, dns = nz // 2, nz // 2 - 1
    return vmem_call(
        functools.partial(layer_kernel, nz, ny, n_x, n_a, n_b),
        [((n_x, rows, wide), BF16)],
        [
            b16(nz, ny, w_rows, 128 * n_a),
            b16(nz, ny, w_rows, 128 * n_b),
            b16(ROWS, wide),
            b16(nz, 2, ROWS, 128),
            b16(ny, 128, ROWS),
            b16(ny, 128, 256),
            b16(nz, 128, 256),
            f32(128, 256),
            f32(ROWS, 256),
            f32(ROWS, ROWS),
            f32(ROWS, 128),
            f32(nz, ny, 128, ROWS),
            f32(ny, nz, ny, 2, ROWS),
            f32(2, ROWS, ROWS),
            f32(2, ROWS, ROWS),
            b16(2, ROWS, ROWS),
            b16(2, ROWS, ROWS),
            f32(128, 128),
            f32(ny, 128, ROWS),
            b16(ny, 128, ROWS),
            b16(ny, 128, ROWS),
            b16(n_x, 2, rows, 256),
            b16(n_x, rows, wide),
            b16(n_x, rows, wide),
            b16(n_x, rows, wide),
            pltpu.SemaphoreType.DMA((n_a + n_b,)),
            sems(ny - 1),
            sems(ups * ny),
            sems(dns * ny),
            sems(ups),
            sems(dns),
            sems(nz),
            sems(nz),
            sems(nz),
            sems(ny - 1),
            sems(ny - 1),
            sems(4 * ups),
            sems(4 * dns),
            sems(2 * ups),
            sems(2 * dns),
            sems((ny - 1) * nz),
            sems(ny - 1),
            sems(1),
            sems(n_x - 1),
        ],
        smem=1,
        cid=1,
        name="layer",
    )(attn_bias, tok, ln_gain, *set_a, *set_b, *rest)[0]


def local(
    nz,
    ny,
    tokens,
    ln_gain,
    w_query_attn,
    w_key_attn,
    w_value_attn,
    w_query_delta,
    w_key_delta,
    w_value_delta,
    w_beta,
    w_decay,
    attn_bias,
    decay_log,
    beta_bias,
    log_decay_extra,
    attn_gain,
    delta_gain,
    w_out_attn,
    w_out_delta,
):
    pieces = layer(
        nz,
        ny,
        lax.axis_size("tp") // 2,
        attn_bias,
        tokens,
        ln_gain[None],
        (w_query_attn, w_key_attn, w_value_attn),
        (w_query_delta, w_key_delta, w_value_delta, w_out_attn.T, w_out_delta.T),
        w_beta.T,
        w_decay.T,
        beta_bias[None],
        decay_log[None],
        log_decay_extra.T,
        delta_gain[None],
        attn_gain[None],
    )
    return jnp.sum(pieces.astype(F32), axis=0).astype(BF16)


def solution(mesh):
    nz, ny = 16, 4
    split = Mesh(mesh.devices.reshape(nz, ny, mesh.shape["tp"]), ("z", "y", "tp"))
    return jax.shard_map(
        functools.partial(local, nz, ny),
        mesh=split,
        in_specs=(
            P(SP, None),
            P(),
            P(SP, "tp"),
            P(SP, "tp"),
            P(SP, "tp"),
            P(SP, "tp"),
            P(SP, "tp"),
            P(SP, "tp"),
            P(),
            P(),
            P(),
            P(),
            P(),
            P(SP, "tp"),
            P(),
            P(),
            P("tp", SP),
            P("tp", SP),
        ),
        out_specs=P(SP + ("tp",), None),
        check_vma=False,
    )
```

```python
import functools

import jax
import jax.numpy as jnp
from jax import lax
from jax.experimental import pallas as pl
from jax.experimental.pallas import tpu as pltpu
from jax.sharding import Mesh
from jax.sharding import PartitionSpec as P

MESH = pl.DeviceIdType.MESH
VMEM = pltpu.VMEM
SP = ("z", "y")
LOG2E = 1.4426950408889634
ROWS = 256
F32 = jnp.float32
BF16 = jnp.bfloat16
HIGH = lax.Precision.HIGHEST


def dot(a, b, dims=((1,), (0,)), precision=None):
    return lax.dot_general(
        a, b, (dims, ((), ())), precision=precision, preferred_element_type=F32
    )


def exact(a, b, dims=((1,), (0,))):
    return dot(a, b, dims, HIGH)


def split(a):
    high = a.astype(BF16)
    return high, (a - high.astype(F32)).astype(BF16)


def close(a, b, dims=((1,), (0,))):
    (ah, al), (bh, bl) = split(a), split(b)
    return dot(ah, bh, dims) + (dot(ah, bl, dims) + dot(al, bh, dims))


def apply_rounded(a, b):
    high, low = split(b)
    return dot(a, high) + dot(a, low)


def vmem_call(body, outs, scratch=(), smem=0, cid=None, name=None):
    params = dict(vmem_limit_bytes=60 * 1024 * 1024)
    if cid is not None:
        params.update(collective_id=cid, has_side_effects=True)

    def call(*args):
        specs = [
            pl.BlockSpec(memory_space=pltpu.SMEM if k < smem else VMEM) for k in range(len(args))
        ]
        return pl.pallas_call(
            body,
            out_shape=tuple(jax.ShapeDtypeStruct(s, d) for s, d in outs),
            in_specs=specs,
            out_specs=tuple(pl.BlockSpec(memory_space=VMEM) for _ in outs),
            scratch_shapes=list(scratch),
            compiler_params=pltpu.CompilerParams(**params),
            name=name,
        )(*args)

    return call


def places(nz, ny):
    z, y, t = lax.axis_index("z"), lax.axis_index("y"), lax.axis_index("tp")

    def at(dz, dy):
        return (lax.rem(z + (dz + nz), nz), lax.rem(y + (dy + ny), ny), t)

    return z, y, at


def remote(src, dst, ssem, rsem, device):
    return pltpu.make_async_remote_copy(
        src_ref=src, dst_ref=dst, send_sem=ssem, recv_sem=rsem, device_id=device, device_id_type=MESH
    )


def meet(peers):
    barrier = pltpu.get_barrier_semaphore()
    for peer in peers:
        pl.semaphore_signal(barrier, inc=1, device_id=peer, device_id_type=MESH)
    pl.semaphore_wait(barrier, len(peers))


class Link:
    def __init__(self, sems, own):
        self.sems, self.own, self.sent = sems, own, []

    def start(self, step, src, dst, device):
        copy = remote(src, dst, self.sems.at[0, step], self.sems.at[1, step], device)
        copy.start()
        self.sent.append(copy)

    def arrived(self, step, dst):
        remote(dst, dst, self.sems.at[0, step], self.sems.at[1, step], self.own).wait_recv()

    def drain(self):
        for copy in self.sent:
            copy.wait_send()


def identity_part():
    rr, cc = iotas((128, 256))
    return jnp.where(rr == cc, 1.0, 0.0), cc < 128


def iotas(shape):
    return lax.broadcasted_iota(jnp.int32, shape, 0), lax.broadcasted_iota(jnp.int32, shape, 1)


def softplus(x):
    return jnp.maximum(x, 0.0) + jnp.log1p(jnp.exp(-jnp.abs(x)))


def sigmoid(x):
    return 1.0 / (1.0 + jnp.exp(-x))


def unit_rows(values):
    return values * lax.rsqrt(jnp.sum(jnp.square(values), axis=-1, keepdims=True) + 1e-06)


SCRATCH = (
    "oa",
    "ob",
    "normed",
    "kvs",
    "qts",
    "mbs",
    "totals",
    "before",
    "solved",
    "qk_part",
    "qd",
    "kept_o",
    "kept_l",
    "s_even",
    "s_odd",
    "w_even",
    "w_odd",
    "state",
    "acc",
    "parts",
    "got",
    "mixed",
    "mine",
    "other",
    "sum_ref",
    "local",
    "ya",
    "za_up",
    "za_dn",
    "zb_up",
    "zb_dn",
    "y_up",
    "y_dn",
    "y_far",
    "y_q",
    "y_m",
    "k_up",
    "k_dn",
    "t_up",
    "t_dn",
    "l_y",
    "y_p",
    "c_p",
    "x_p",
)


def layer_kernel(nz, ny, n_x, n_a, n_b, attn_bias, tok, ln_gain, *refs):
    n = n_a + n_b
    ins, refs = refs[:n], refs[n:]
    w_beta, w_decay, beta_bias, decay_log, extra, delta_gain, attn_gain, seen = refs[:8]
    r_ = dict(zip(SCRATCH, refs[8:]))
    oa, ob, normed_ref, kvs, qts, mbs, totals, before, solved, qk, qd = [
        r_[k] for k in SCRATCH[:11]
    ]
    kept_o, kept_l, s_even, s_odd, w_even, w_odd = [r_[k] for k in SCRATCH[11:17]]
    state, acc, parts, got, mixed, mine, other, sum_ref, local = [r_[k] for k in SCRATCH[17:26]]
    z, y, at = places(nz, ny)
    t = lax.axis_index("tp")
    x, c = lax.div(t, 2), lax.rem(t, 2)
    up, down, left, right = at(1, 0), at(-1, 0), at(0, -1), at(0, 1)
    row = lambda d: lax.rem(z + (d + nz), nz)
    col = lambda d: lax.rem(y + (d + ny), ny)
    far = lambda d: lax.rem(x + (d + n_x), n_x)
    in_y = lambda d: at(0, d)
    twin = (z, y, 2 * x + (1 - c))
    in_x = lambda d: (z, y, 2 * far(d) + c)
    ups, dns = nz // 2, nz // 2 - 1
    every = {k: Link(r_[k], twin) for k in SCRATCH[26:]}
    links = [every[k] for k in SCRATCH[26:] if k not in ("k_up", "k_dn")]
    ya, za_up, za_dn, zb_up, zb_dn, y_up, y_dn, y_far = [every[k] for k in SCRATCH[26:34]]
    y_q, y_m, k_up, k_dn, t_up, t_dn, l_y, y_p, c_p, x_p = [every[k] for k in SCRATCH[34:]]
    packs = []
    for k in range(n):
        out, place = (oa, k) if k < n_a else (ob, k - n_a)
        dst = out.at[z, y, :, pl.ds(128 * place, 128)]
        packs.append(pltpu.make_async_copy(ins[k], dst, local.at[k]))
        packs[-1].start()
    meet(
        [up, down]
        + [in_y(d) for d in range(1, ny)]
        + [twin]
        + [in_x(d) for d in range(1, n_x)]
    )
    for pack in packs:
        pack.wait()
    order = (0, 3, 1, 2)
    for d in (1, 3, 2):
        ya.start(d - 1, oa.at[z, y], oa.at[z, y], at(0, d))

    def lead(c):
        block = oa.at[z, col(c)]
        za_up.start(c, block, block, up)
        za_dn.start(c, block, block, down)

    def fan(k, zz):
        y_up.start(k, ob.at[zz, y], ob.at[zz, y], right)
        y_dn.start(k, ob.at[zz, y], ob.at[zz, y], left)

    def relay(k, zz):
        y_up.arrived(k, ob.at[zz, col(-1)])
        y_dn.arrived(k, ob.at[zz, col(1)])
        if k % 2 == 0:
            y_far.start(k, ob.at[zz, col(-1)], ob.at[zz, col(-1)], right)
        else:
            y_far.start(k, ob.at[zz, col(1)], ob.at[zz, col(1)], left)

    lead(0)
    zb_up.start(0, ob.at[z, y], ob.at[z, y], up)
    zb_dn.start(0, ob.at[z, y], ob.at[z, y], down)
    fan(0, z)
    values = tok[...].astype(F32)
    center = jnp.mean(values, axis=-1, keepdims=True)
    shifted = values - center
    spread = jnp.mean(jnp.square(shifted), axis=-1, keepdims=True)
    normed_ref[...] = (shifted * lax.rsqrt(spread + 1e-05) * ln_gain[...]).astype(BF16)
    for c_ in order[1:]:
        ya.arrived(ny - c_ - 1, oa.at[z, col(c_)])
        lead(c_)
    waiting = [(0, z)]
    ways = ((-1, ups, zb_up, za_up, up), (1, dns, zb_dn, za_dn, down))
    for s in range(ups):
        fresh = []
        for c_ in order:
            for sign, steps, zb, za, to in ways:
                if s >= steps:
                    continue
                zz = row(sign * (s + 1))
                za.arrived(s * ny + c_, oa.at[zz, col(c_)])
                if s + 1 < steps:
                    za.start((s + 1) * ny + c_, oa.at[zz, col(c_)], oa.at[zz, col(c_)], to)
                if c_ == 0:
                    zb.arrived(s, ob.at[zz, y])
                    if s + 1 < steps:
                        zb.start(s + 1, ob.at[zz, y], ob.at[zz, y], to)
                    k = 2 * s + (1 if sign < 0 else 2)
                    fan(k, zz)
                    fresh.append((k, zz))
        for k, zz in waiting:
            relay(k, zz)
        waiting = fresh
    for k, zz in waiting:
        relay(k, zz)

    normed = normed_ref[...]
    weights_a = oa[...].reshape(-1, 128 * n_a)
    attn = dot(normed, weights_a).astype(BF16)
    qts[y] = jnp.transpose(attn[:, :128].astype(F32)).astype(BF16)
    r, c_ = iotas((ROWS, ROWS))
    shuffle = jnp.where(c_ == (r & 7) * (ROWS // 8) + (r >> 3), 1.0, 0.0).astype(BF16)
    kvs[z, 0] = dot(shuffle, attn[:, 128:256]).astype(BF16)
    kvs[z, 1] = dot(shuffle, attn[:, 256:384]).astype(BF16)
    beta_pre = dot(normed, w_beta[...], ((1,), (1,))).astype(BF16).astype(F32)
    decay_pre = dot(normed, w_decay[...], ((1,), (1,))).astype(BF16).astype(F32)
    for k in range(nz):
        y_far.arrived(k, ob.at[z, col(2)])
    half = ROWS // 2
    part = lambda ref, p: ref.at[lax.div(p, 2), pl.ds(half * lax.rem(p, 2), half)]
    for d in (1, 3, 2):
        y_q.start(d - 1, qts.at[y], qts.at[y], in_y(d))
    for p in range(4):
        for link, to in ((k_up, up), (k_dn, down)):
            block = kvs.at[z, p // 2, pl.ds(half * (p % 2), half)]
            remote(block, block, link.sems.at[0, p], link.sems.at[1, p], to).start()
    delta = dot(normed, ob[:, :, :, : 3 * 128].reshape(-1, 384)).astype(BF16).astype(F32)

    groups = ROWS // 8
    sub = lax.broadcasted_iota(jnp.int32, (8, ROWS), 0)
    query = lax.broadcasted_iota(jnp.int32, (8, ROWS), 1)

    def score(zp, yq, s):
        for h in range(2):
            s[h] = dot(kvs[zp, 0, :, h * 64 : h * 64 + 64], qts[yq, h * 64 : h * 64 + 64, :])

    def weigh(zp, yq, s, w, masked=False):
        ahead = query + ROWS * (yq - y)
        sums = []
        for h in range(2):
            run = jnp.zeros((8, ROWS), F32)
            left = [None] * groups
            for g in reversed(range(groups)):
                u = s[h, g * 8 : g * 8 + 8, :] * (0.125 * LOG2E) + attn_bias[2 * t + h] * LOG2E
                lost = jnp.maximum(u, jnp.log2(1.0 + jnp.exp2(jnp.minimum(u, 100.0))))
                if masked:
                    lost = jnp.where(sub * groups + g < ahead, lost, 0.0)
                run = run + lost
                left[g] = u - run
            incl = run
            for d in (1, 2, 4):
                incl = incl + jnp.where(sub < 8 - d, pltpu.roll(incl, 8 - d, 0), 0.0)
            later = jnp.where(sub < 7, pltpu.roll(incl, 7, 0), 0.0)
            for g in range(0, groups, 2):
                pair = [jnp.exp2(left[j] - later) for j in (g, g + 1)]
                if masked:
                    pair = [
                        jnp.where(sub * groups + j < ahead, e, 0.0) for e, j in zip(pair, (g, g + 1))
                    ]
                w[h, g * 8 : g * 8 + 16, :] = jnp.concatenate(pair, axis=0).astype(BF16)
            sums.append(incl[:1])
        kept_l[y, zp, yq] = jnp.concatenate(sums, axis=0)

    def apply(zp, yq, w):
        for h in range(2):
            kept_o[zp, yq, h * 64 : h * 64 + 64, :] = dot(
                kvs[zp, 1, :, h * 64 : h * 64 + 64], w[h], ((0,), (0,))
            )

    def send_sums(block, zz):
        for d in (1, 3, 2):
            l_y.start(3 * block + d - 1, kept_l.at[y, zz], kept_l.at[y, zz], in_y(d))

    def forward(s, p):
        for sign, steps, link, to in ((-1, ups, k_up, up), (1, dns, k_dn, down)):
            if s < steps:
                block = part(kvs.at[row(sign * (s + 1))], p)
                link.arrived(4 * s + p, block)
                if s + 1 < steps:
                    step = 4 * (s + 1) + p
                    remote(block, block, link.sems.at[0, step], link.sems.at[1, step], to).start()

    t_rows = totals.shape[1] // 2
    piece = lambda zz, p: totals.at[zz, pl.ds(t_rows * p, t_rows)]

    def forward_totals(j):
        for sign, steps, link, to in ((-1, ups, t_up, up), (1, dns, t_dn, down)):
            if j < steps:
                zz = row(sign * (j + 1))
                for p in range(2):
                    link.arrived(2 * j + p, piece(zz, p))
                    if j + 1 < steps:
                        link.start(2 * (j + 1) + p, piece(zz, p), piece(zz, p), to)

    lane = lax.broadcasted_iota(jnp.int32, (1, w_beta.shape[0]), 1)

    def pick(a):
        return jnp.sum(jnp.where(lane == t, a, 0.0), axis=-1, keepdims=True)

    beta = sigmoid(pick(beta_pre) + pick(beta_bias[...]))
    rate = jnp.exp(pick(decay_log[...]))
    added = jnp.transpose(jnp.broadcast_to(extra[...], (8, ROWS)))[:, :1]
    decay = -rate * softplus(pick(decay_pre)) + added
    silu = delta * sigmoid(delta)
    queries = unit_rows(silu[:, :128]) * (128.0**-0.5)
    keys = unit_rows(silu[:, 128:256])
    vals = silu[:, 256:]
    lower = r >= c_
    total = exact(jnp.where(lower, 1.0, 0.0), jnp.broadcast_to(decay, (ROWS, 128)))
    across = jnp.transpose(total)[:1, :]
    total = total[:, :1]
    end = total[ROWS - 1 :, :]
    mask = jnp.where(lower, jnp.exp(jnp.where(lower, total - across, 0.0)), 0.0)
    keys_beta = keys * beta
    grown = jnp.exp(total)
    nmat = jnp.where(r > c_, close(keys_beta, keys, ((1,), (1,))) * mask, 0.0)
    r6, c6 = iotas((64, 64))
    cuts = [slice(64 * b, 64 * b + 64) for b in range(ROWS // 64)]
    own_n = [nmat[b, b] for b in cuts]
    near = [jnp.where((r6 >> 3) == (c6 >> 3), m, 0.0) for m in own_n]
    two = [close(m, m) for m in near]
    four = [close(m, m) for m in two]
    invs = [jnp.where(r6 == c6, 1.0, 0.0) - m for m in near]
    invs = [a + close(a, m) for a, m in zip(invs, two)]
    invs = [a + close(a, m) for a, m in zip(invs, four)]
    for bit in range(3, 6):
        cross = ((r6 >> (bit + 1)) == (c6 >> (bit + 1))) & ((r6 >> bit) != (c6 >> bit))
        bands = [jnp.where(cross, m, 0.0) for m in own_n]
        bands = [close(m, a) for m, a in zip(bands, invs)]
        invs = [a - close(a, m) for a, m in zip(invs, bands)]
    inv = jnp.concatenate([jnp.concatenate([a] * len(cuts), axis=1) for a in invs], axis=0)
    inv = jnp.where((r >> 6) == (c_ >> 6), inv, 0.0)

    @pl.loop(0, 4)
    def _(p):
        forward(0, p)

    for bit in range(6, 8):
        cross = ((r >> (bit + 1)) == (c_ >> (bit + 1))) & ((r >> bit) != (c_ >> bit))
        band = jnp.where(cross, nmat, 0.0)
        inv = inv - close(inv, close(band, inv))
    answer = close(inv, jnp.concatenate([keys_beta * grown, vals * beta], axis=1))
    solved[...] = answer
    to_end = keys * jnp.exp(end - total)
    written = close(to_end, answer, ((0,), (0,)))
    eye, left_half = identity_part()
    mbs[y] = jnp.where(left_half, eye * (jnp.exp(end) - 1.0) - written, written).astype(BF16)
    qk[...] = close(queries, keys, ((1,), (1,))) * mask
    qd[...] = queries * grown
    for d in (1, 3, 2):
        y_m.start(d - 1, mbs.at[y], mbs.at[y], in_y(d))

    for d in (1, 3, 2):
        y_q.arrived(d - 1, qts.at[col(-d)])
    w_odd[...] = jnp.zeros_like(w_odd)
    score(z, 0, s_even)

    @pl.loop(0, ny // 2)
    def _(m):
        yq = 2 * m
        score(z, yq + 1, s_odd)
        weigh(z, yq, s_even, w_even, True)
        apply(z, jnp.maximum(yq - 1, 0), w_odd)
        score(z, jnp.minimum(yq + 2, ny - 1), s_even)
        weigh(z, yq + 1, s_odd, w_odd, True)
        apply(z, yq, w_even)

    apply(z, ny - 1, w_odd)
    score(row(-1), 0, s_even)

    for s in range(1, ups):
        if s == 1:
            for d in (1, 3, 2):
                y_m.arrived(d - 1, mbs.at[col(-d)])
            eye, left_half = identity_part()
            chain, first = eye, eye
            for k in range(ny):
                m = mbs[k]
                first = jnp.where(y == k, chain, first)
                shift = chain + jnp.where(left_half, 0.0, m.astype(F32))
                chain = apply_rounded(m[:, :128], chain) + shift
            before[...] = first
            totals[z] = (chain - eye).astype(BF16)
        one, two = row(-s), row(s)
        last = two if s == 1 else row(s - 1)
        ahead = row(-s - 1)

        @pl.loop(0, ny)
        def _(p):
            forward(s, p)
            at_start, at_end = p == 0, p == ny - 1
            score(two, p, s_odd)
            weigh(one, p, s_even, w_even)
            apply(jnp.where(at_start, last, two), lax.rem(p + ny - 1, ny), w_odd)
            score(jnp.where(at_end, ahead, one), lax.rem(p + 1, ny), s_even)
            weigh(two, p, s_odd, w_odd)
            apply(one, p, w_even)

        if s == 1:
            for p in range(2):
                t_up.start(p, piece(z, p), piece(z, p), up)
                t_dn.start(p, piece(z, p), piece(z, p), down)
            send_sums(0, z)
        else:
            forward_totals(s - 2)
            send_sums(2 * s - 3, row(1 - s))
            send_sums(2 * s - 2, row(s - 1))

    one, two = row(-ups), row(ups - 1)
    score(one, 1, s_odd)
    weigh(one, 0, s_even, w_even)
    apply(two, ny - 1, w_odd)
    send_sums(2 * ups - 3, row(1 - ups))
    send_sums(2 * ups - 2, row(ups - 1))
    forward_totals(ups - 2)
    score(one, 2, s_even)
    weigh(one, 1, s_odd, w_odd)
    apply(one, 0, w_even)
    score(one, 3, s_odd)
    weigh(one, 2, s_even, w_even)
    apply(one, 1, w_odd)
    weigh(one, 3, s_odd, w_odd)
    apply(one, 2, w_even)
    apply(one, 3, w_odd)
    forward_totals(ups - 1)
    send_sums(2 * ups - 1, one)

    state[...] = jnp.zeros_like(state)

    @pl.loop(0, z)
    def _(k):
        now = state[...]
        state[...] = now + apply_rounded(totals[k, :, :128], now) + totals[k, :, 128:].astype(F32)

    incoming = close(before[:, :128], state[...]) + before[:, 128:]
    fresh = solved[:, 128:] - close(solved[:, :128], incoming)
    raw = close(qd[...], incoming) + close(qk[...], fresh)
    scale = lax.rsqrt(jnp.mean(jnp.square(raw), axis=-1, keepdims=True) + 1e-06)
    rows = seen.shape[1]
    delta = (raw * scale * delta_gain[...]).astype(BF16)
    mixed[:, :, :, 128:] = delta.reshape(n_x, 2, rows, 128)

    blocks = [(0, z)] + [(1 + 2 * j, row(-1 - j)) for j in range(ups)]
    blocks += [(2 + 2 * j, row(1 + j)) for j in range(dns)]
    for block, zz in blocks:
        for d in (1, 3, 2):
            l_y.arrived(3 * block + d - 1, kept_l.at[col(-d), zz])
    acc[...] = jnp.zeros_like(acc)

    def rescale(i, later):
        zp = z - i
        sums = [kept_l[k, zp] for k in range(ny)]
        here = later
        for k in range(ny):
            here = here + jnp.where(k > y, sums[k], 0.0)
            later = later + sums[k]
        kept = jnp.exp2(-here)
        for yq in range(ny):
            for h in range(2):
                part_rows = slice(h * 64, h * 64 + 64)
                acc[yq, part_rows, :] += kept_o[zp, yq, part_rows, :] * kept[yq, h : h + 1, :]
        return later

    lax.fori_loop(0, z + 1, rescale, jnp.zeros(kept_l.shape[2:], F32))
    parts[...] = acc[...].astype(BF16)
    raw = acc[y]
    for d in (1, 3, 2):
        y_p.start(d - 1, parts.at[col(d)], got.at[y], in_y(d))
    for d in (1, 3, 2):
        y_p.arrived(d - 1, got.at[col(-d)])
        raw = raw + got[col(-d)].astype(F32)
    halves = []
    for h in range(2):
        piece_h = raw[h * 64 : h * 64 + 64]
        power = jnp.mean(jnp.square(piece_h), axis=0, keepdims=True)
        halves.append(piece_h * lax.rsqrt(power + 1e-06))
    gains = jnp.concatenate([attn_gain[...], attn_gain[...]], axis=1)
    attn = (jnp.transpose(jnp.concatenate(halves, axis=0)) * gains).astype(BF16)
    mixed[:, :, :, :128] = attn.reshape(n_x, 2, rows, 128)

    def product(core):
        picked = mixed[:, core].reshape(n_x * rows, 256)
        return dot(picked, ob[:, :, :, 3 * 128 :].reshape(-1, 256), ((1,), (1,))).astype(BF16).reshape(n_x, rows, -1)

    mine[...] = product(1 - c)
    own = product(c)
    c_p.start(0, mine, other, twin)
    sum_ref[...] = own
    c_p.arrived(0, other)
    for d in (2, 1, 3):
        sum_ref[far(d)] = (sum_ref[far(d)].astype(F32) + other[far(d)].astype(F32)).astype(BF16)
    seen[x] = (sum_ref[x].astype(F32) + other[x].astype(F32)).astype(BF16)
    for d in (2, 1, 3):
        x_p.start(d - 1, sum_ref.at[far(d)], seen.at[x], in_x(d))
    for d in (1, 3, 2):
        x_p.arrived(d - 1, seen.at[far(-d)])
    for link in links:
        link.drain()
    for link, steps in ((k_up, ups), (k_dn, dns)):

        @pl.loop(0, 4 * steps)
        def _(k):
            block = part(kvs.at[z], lax.rem(k, 4))
            remote(block, block, link.sems.at[0, k], link.sems.at[1, k], twin).wait_send()


def layer(nz, ny, n_x, attn_bias, tok, ln_gain, set_a, set_b, *rest):
    n_a, n_b = len(set_a), len(set_b)
    w_rows, wide = set_a[0].shape[0], nz * ny * set_a[0].shape[0]
    rows = ROWS // (2 * n_x)
    sems = lambda n: pltpu.SemaphoreType.DMA((2, n))
    f32 = lambda *shape: pltpu.VMEM(shape, F32)
    b16 = lambda *shape: pltpu.VMEM(shape, BF16)
    ups, dns = nz // 2, nz // 2 - 1
    return vmem_call(
        functools.partial(layer_kernel, nz, ny, n_x, n_a, n_b),
        [((n_x, rows, wide), BF16)],
        [
            b16(nz, ny, w_rows, 128 * n_a),
            b16(nz, ny, w_rows, 128 * n_b),
            b16(ROWS, wide),
            b16(nz, 2, ROWS, 128),
            b16(ny, 128, ROWS),
            b16(ny, 128, 256),
            b16(nz, 128, 256),
            f32(128, 256),
            f32(ROWS, 256),
            f32(ROWS, ROWS),
            f32(ROWS, 128),
            f32(nz, ny, 128, ROWS),
            f32(ny, nz, ny, 2, ROWS),
            f32(2, ROWS, ROWS),
            f32(2, ROWS, ROWS),
            b16(2, ROWS, ROWS),
            b16(2, ROWS, ROWS),
            f32(128, 128),
            f32(ny, 128, ROWS),
            b16(ny, 128, ROWS),
            b16(ny, 128, ROWS),
            b16(n_x, 2, rows, 256),
            b16(n_x, rows, wide),
            b16(n_x, rows, wide),
            b16(n_x, rows, wide),
            pltpu.SemaphoreType.DMA((n_a + n_b,)),
            sems(ny - 1),
            sems(ups * ny),
            sems(dns * ny),
            sems(ups),
            sems(dns),
            sems(nz),
            sems(nz),
            sems(nz),
            sems(ny - 1),
            sems(ny - 1),
            sems(4 * ups),
            sems(4 * dns),
            sems(2 * ups),
            sems(2 * dns),
            sems((ny - 1) * nz),
            sems(ny - 1),
            sems(1),
            sems(n_x - 1),
        ],
        smem=1,
        cid=1,
        name="layer",
    )(attn_bias, tok, ln_gain, *set_a, *set_b, *rest)[0]


def local(
    nz,
    ny,
    tokens,
    ln_gain,
    w_query_attn,
    w_key_attn,
    w_value_attn,
    w_query_delta,
    w_key_delta,
    w_value_delta,
    w_beta,
    w_decay,
    attn_bias,
    decay_log,
    beta_bias,
    log_decay_extra,
    attn_gain,
    delta_gain,
    w_out_attn,
    w_out_delta,
):
    pieces = layer(
        nz,
        ny,
        lax.axis_size("tp") // 2,
        attn_bias,
        tokens,
        ln_gain[None],
        (w_query_attn, w_key_attn, w_value_attn),
        (w_query_delta, w_key_delta, w_value_delta, w_out_attn.T, w_out_delta.T),
        w_beta.T,
        w_decay.T,
        beta_bias[None],
        decay_log[None],
        log_decay_extra.T,
        delta_gain[None],
        attn_gain[None],
    )
    return jnp.sum(pieces.astype(F32), axis=0).astype(BF16)


def solution(mesh):
    nz, ny = 16, 4
    split = Mesh(mesh.devices.reshape(nz, ny, mesh.shape["tp"]), ("z", "y", "tp"))
    return jax.shard_map(
        functools.partial(local, nz, ny),
        mesh=split,
        in_specs=(
            P(SP, None),
            P(),
            P(SP, "tp"),
            P(SP, "tp"),
            P(SP, "tp"),
            P(SP, "tp"),
            P(SP, "tp"),
            P(SP, "tp"),
            P(),
            P(),
            P(),
            P(),
            P(),
            P(SP, "tp"),
            P(),
            P(),
            P("tp", SP),
            P("tp", SP),
        ),
        out_specs=P(SP + ("tp",), None),
        check_vma=False,
    )
```
